32 devices in a mesh: fs: 8 (over z, x), tp: 4 (over y, core).
Axes of the slice: x: 2, y: 2, z: 4, core: 2. Of those that a mesh axis runs over, the one named last changes fastest.
Arguments:
- prompts: bfloat16 [4, 1024, 2048], P('tp'), may hold values from -6 to 6
- gain_first: float32 [2048], P('fs'), may hold values from 0.1 to 1.9
- gate_first: float32 [2048, 5632], P('fs', 'tp'), may hold values from -0.125 to 0.125
- up_first: float32 [2048, 5632], P('fs', 'tp'), may hold values from -0.125 to 0.125
- down_first: float32 [5632, 2048], P('fs', 'tp'), may hold values from -0.078125 to 0.078125
- gain_second: float32 [2048], P('fs'), may hold values from 0.1 to 1.9
- gate_second: float32 [2048, 5632], P('fs', 'tp'), may hold values from -0.125 to 0.125
- up_second: float32 [2048, 5632], P('fs', 'tp'), may hold values from -0.125 to 0.125
- down_second: float32 [5632, 2048], P('fs', 'tp'), may hold values from -0.078125 to 0.078125
Outputs:
- served_gate_first: bfloat16 [2048, 5632], P(None, 'fs')
- served_up_first: bfloat16 [2048, 5632], P(None, 'fs')
- served_down_first: bfloat16 [5632, 2048], P('fs')
- served_gate_second: bfloat16 [2048, 5632], P(None, 'fs')
- served_up_second: bfloat16 [2048, 5632], P(None, 'fs')
- served_down_second: bfloat16 [5632, 2048], P('fs')
- prompt_states: bfloat16 [4, 1024, 2048], P('tp', 'fs')
The draws below stay inside these ranges and needn't reach their ends.
All inputs are finite; a program needn't handle non-finite values.
Results may differ from the reference program's by a relative error of at most 0.012.
Values may be sent and summed in bfloat16 or wider, within the bound.
A program may use at most 128 MiB of HBM per device.

```python
import jax
import jax.numpy as jnp
from jax import lax

D = 2048
FF = 5632
PLEN = 1024
PROMPTS = 4
N_FS = 8


def levels(rng, dims, cuts, smallest, top_value):
    gain, own = 1.0, jax.random.fold_in(rng, 6)
    for dim, parts in cuts:
        draws = jnp.exp(jax.random.uniform(jax.random.fold_in(own, dim), (parts,), jnp.float32, smallest / len(cuts), top_value / len(cuts)))
        gain = gain * jnp.repeat(draws, dims[dim] // parts).reshape([-1 if axis == dim else 1 for axis in range(len(dims))])
    return gain


def bell_draw(own_key, dims, spread, bound, split=(), held_as=jnp.bfloat16):
    factor_of = levels(own_key, dims, split, -0.22, 0.18) if split else 1.0
    result = jax.random.normal(own_key, dims, jnp.float32) * spread * factor_of
    return jnp.minimum(jnp.maximum(result, -bound), bound).astype(held_as)


def setup_inputs(seed: int = 0) -> dict:
    splits = jax.random.split(jax.random.key(seed), 10)
    prompts = bell_draw(splits[0], (PROMPTS, PLEN, D), 1.0, 6.0, ((0, 4),))
    gain_first = jnp.clip(1.0 + 0.18 * jax.random.normal(splits[1], (D,), jnp.float32), 0.1, 1.9)
    gate_first = bell_draw(splits[2], (D, FF), D ** -0.5, 0.125, ((0, 8), (1, 4)), jnp.float32)
    up_first = bell_draw(splits[3], (D, FF), D ** -0.5, 0.125, ((0, 8), (1, 4)), jnp.float32)
    down_first = bell_draw(splits[4], (FF, D), FF ** -0.5, 0.078125, ((0, 8), (1, 4)), jnp.float32)
    gain_second = jnp.clip(1.0 + 0.18 * jax.random.normal(splits[5], (D,), jnp.float32), 0.1, 1.9)
    gate_second = bell_draw(splits[6], (D, FF), D ** -0.5, 0.125, ((0, 8), (1, 4)), jnp.float32)
    up_second = bell_draw(splits[7], (D, FF), D ** -0.5, 0.125, ((0, 8), (1, 4)), jnp.float32)
    down_second = bell_draw(splits[8], (FF, D), FF ** -0.5, 0.078125, ((0, 8), (1, 4)), jnp.float32)
    return dict(prompts=prompts, gain_first=gain_first, gate_first=gate_first, up_first=up_first, down_first=down_first, gain_second=gain_second, gate_second=gate_second, up_second=up_second, down_second=down_second)


def normalize(row_block):
    widened = row_block.astype(jnp.float32)
    scaled = widened * lax.rsqrt(lax.optimization_barrier(jnp.mean(widened * widened, axis=-1, keepdims=True)) + 1e-06)
    return scaled.astype(jnp.bfloat16)

def block_sum(active, down_rows):
    unit_count = active.shape[1] // N_FS

    def advance(running, block_index):
        left_cols = lax.dynamic_slice_in_dim(active, block_index * unit_count, unit_count, 1)
        right_rows = lax.dynamic_slice_in_dim(down_rows, block_index * unit_count, unit_count, 0)
        partial_sum = jnp.dot(left_cols, right_rows, preferred_element_type=jnp.float32).astype(jnp.bfloat16)
        partial_sum = lax.optimization_barrier(partial_sum)
        return (running + partial_sum.astype(jnp.float32), None)
    start_sum = jnp.zeros((active.shape[0], down_rows.shape[1]), jnp.float32)
    running, _ = lax.scan(advance, start_sum, jnp.arange(N_FS, dtype=jnp.int32))
    return running

def half_step(tokens_in, gate_cols, up_cols, down_rows):
    normed = normalize(tokens_in)
    gate_val = jnp.dot(normed, gate_cols, preferred_element_type=jnp.float32)
    up_val = jnp.dot(normed, up_cols, preferred_element_type=jnp.float32)
    active = (jax.nn.silu(gate_val) * up_val).astype(jnp.bfloat16)
    branch = block_sum(active, down_rows)
    return (tokens_in.astype(jnp.float32) + 0.5 * branch).astype(jnp.bfloat16)

def reference(prompts, gain_first, gate_first, up_first, down_first, gain_second, gate_second, up_second, down_second):
    served_gate_first = (gain_first[:, None] * gate_first).astype(jnp.bfloat16)
    served_up_first = (gain_first[:, None] * up_first).astype(jnp.bfloat16)
    served_gate_second = (gain_second[:, None] * gate_second).astype(jnp.bfloat16)
    served_up_second = (gain_second[:, None] * up_second).astype(jnp.bfloat16)
    served_down_first = down_first.astype(jnp.bfloat16)
    served_down_second = down_second.astype(jnp.bfloat16)
    tokens_in = prompts.reshape(-1, prompts.shape[-1])
    middle = half_step(tokens_in, served_gate_first, served_up_first, served_down_first)
    finished = half_step(middle, served_gate_second, served_up_second, served_down_second)
    return (served_gate_first, served_up_first, served_down_first, served_gate_second, served_up_second, served_down_second, finished.reshape(prompts.shape))
```

```python
import functools

import jax
import jax.numpy as jnp
from jax import lax
from jax.experimental import pallas as pl
from jax.experimental.pallas import tpu as pltpu
from jax.sharding import PartitionSpec as P

CORES = 2
CUTS = 2
TILE = 256


def partner(index, step, count):
    if count & (count - 1):
        return (index + step) % count
    result, bit = 0, 1
    while bit < count:
        result = result + ((index // bit + step // bit) % 2) * bit
        bit *= 2
    return result


def tiles(total, size):
    return [(start, min(size, total - start)) for start in range(0, total, size)]


class Ring:
    def __init__(self, n_z, n_x):
        self.n_z, self.n_x, self.n = n_z, n_x, n_z * n_x

    def position(self, z, x):
        if self.n_x == 1:
            return z
        row, wide = self.n_z - 1 - z, self.n_x - 1
        back = self.n_z + row * wide + jnp.where(row % 2 == 0, x - 1, self.n_x - 1 - x)
        return jnp.where(x == 0, z, back)

    def at(self, place):
        place = (place + self.n) % self.n
        if self.n_x == 1:
            return place
        wide = self.n_x - 1
        rest = place + self.n - self.n_z
        row = (rest - self.n) // wide
        col = (rest - self.n) % wide
        back = (self.n_z - 1 - row) * self.n_x + jnp.where(row % 2 == 0, 1 + col, self.n_x - 1 - col)
        return jnp.where(place < self.n_z, place * self.n_x, back)

    def slot(self, offset):
        offset = offset % self.n
        if offset == 0:
            return 0
        if 2 * offset == self.n:
            return 1
        return 2 * offset + 1 if 2 * offset < self.n else 2 * (self.n - offset)


def remote(src, dst, send, recv, f, t):
    return pltpu.make_async_remote_copy(
        src_ref=src, dst_ref=dst, send_sem=send, recv_sem=recv,
        device_id={"fs": f, "tp": t}, device_id_type=pl.DeviceIdType.MESH,
    )


class Exchange:
    def __init__(self, n_fs, n_tp, gu, dn, gu_out, dn_out, sems):
        (self.send_a, self.recv_a, self.send_y, self.recv_y, self.send_m, self.recv_m,
         self.dn_local, self.dn_send_y, self.dn_recv_y, self.dn_send_m, self.dn_recv_m) = sems
        self.n_fs, self.n_tp, self.n_y = n_fs, n_tp, n_tp // CORES
        self.per = n_fs // n_tp
        self.gu, self.dn, self.gu_out, self.dn_out = gu, dn, gu_out, dn_out
        self.hidden, self.rows = gu.shape[1] // self.per, gu.shape[2]
        self.part = self.hidden // self.n_y
        self.me_f, self.me_t = lax.axis_index("fs"), lax.axis_index("tp")
        self.my_y, self.my_c = self.me_t // CORES, self.me_t % CORES
        self.mate = self.my_y * CORES + (1 - self.my_c)
        self.sends = []

    def peer(self, step):
        return (self.my_y + step) % self.n_y

    def window(self, f, y, c):
        return self.gu_out.at[c, pl.ds(pl.multiple_of(y * self.part, 8), self.part),
                              pl.ds(pl.multiple_of(f * self.rows, 128), self.rows)]

    def first(self, i, step):
        q = (self.me_t + step) % self.n_tp
        y, c = q // CORES, q % CORES
        f = self.me_t * self.per + i
        src = self.gu.at[c, pl.ds(pl.multiple_of(i * self.hidden + y * self.part, 8), self.part), :]
        dst = self.window(self.me_f, y, c)
        copy = remote(src, dst, self.send_a.at[i * self.n_tp + step], self.recv_a.at[self.me_f], f, q)
        return copy, src, dst, f == self.me_f

    def start_gu(self):
        for step in range(self.n_tp - 1, -1, -1):
            for i in range(self.per):
                copy, src, dst, here = self.first(i, step)
                if step == 0:
                    @pl.when(here)
                    def _():
                        pltpu.make_async_copy(src, dst, self.recv_a.at[self.me_f]).start()

                    @pl.when(jnp.logical_not(here))
                    def _():
                        copy.start()
                else:
                    copy.start()

    def columns(self, t):
        width = self.dn.shape[1]
        return self.dn_out.at[:, pl.ds(pl.multiple_of(t * width, 128), width)]

    def start_dn(self):
        mine = self.columns(self.me_t)
        self.keep = pltpu.make_async_copy(self.dn, mine, self.dn_local)
        self.keep.start()
        for step in range(1, self.n_y):
            self.sends.append(remote(self.dn, mine, self.dn_send_y.at[step], self.dn_recv_y.at[self.my_y],
                                     self.me_f, self.peer(step) * CORES + self.my_c))
            self.sends[-1].start()
        self.sends.append(remote(self.dn, mine, self.dn_send_m.at[0], self.dn_recv_m.at[self.my_y],
                                 self.me_f, self.mate))
        self.sends[-1].start()

    def pass_first(self):
        for step in range(self.n_fs):
            f = partner(self.me_f, step, self.n_fs)
            piece = self.window(f, self.my_y, self.my_c)
            slot = self.my_y * self.n_fs + f
            remote(piece, piece, self.send_m.at[0], self.recv_a.at[f], self.me_f, self.mate).wait_recv()
            for hop in range(1, self.n_y):
                self.sends.append(remote(piece, piece, self.send_y.at[(hop - 1) * self.n_fs + step],
                                         self.recv_y.at[slot], self.me_f, self.peer(hop) * CORES + self.my_c))
                self.sends[-1].start()
            self.sends.append(remote(piece, piece, self.send_m.at[step], self.recv_m.at[slot],
                                     self.me_f, self.mate))
            self.sends[-1].start()

    def pass_dn(self):
        for hop in range(1, self.n_y):
            y = self.peer(hop)
            block = self.columns(y * CORES + self.my_c)
            copy = remote(block, block, self.dn_send_m.at[hop], self.dn_recv_m.at[y], self.me_f, self.mate)
            remote(block, block, self.dn_send_m.at[hop], self.dn_recv_y.at[y], self.me_f, self.mate).wait_recv()
            copy.start()
            self.sends.append(copy)

    def pass_second(self):
        for step in range(self.n_fs):
            f = partner(self.me_f, step, self.n_fs)
            for hop in range(1, self.n_y):
                y = self.peer(hop)
                piece = self.window(f, y, self.my_c)
                send = self.send_m.at[hop * self.n_fs + step]
                slot = y * self.n_fs + f
                remote(piece, piece, send, self.recv_y.at[slot], self.me_f, self.mate).wait_recv()
                self.sends.append(remote(piece, piece, send, self.recv_m.at[slot], self.me_f, self.mate))
                self.sends[-1].start()

    def arrive_gu(self):
        for hop in range(self.n_y):
            y = self.peer(hop)
            for step in range(self.n_fs):
                f = partner(self.me_f, step, self.n_fs)
                piece = self.window(f, y, 1 - self.my_c)
                remote(piece, piece, self.send_m.at[0], self.recv_m.at[y * self.n_fs + f],
                       self.me_f, self.mate).wait_recv()

    def arrive_dn(self):
        for hop in range(self.n_y):
            y = self.peer(hop)
            block = self.columns(y * CORES + (1 - self.my_c))
            remote(block, block, self.dn_send_m.at[0], self.dn_recv_m.at[y], self.me_f, self.mate).wait_recv()
        self.keep.wait()

    def drain(self):
        for copy in self.sends:
            copy.wait_send()
        for i in range(self.per):
            for step in range(self.n_tp):
                copy, _, _, here = self.first(i, step)
                if step == 0:
                    @pl.when(jnp.logical_not(here))
                    def _():
                        copy.wait_send()
                else:
                    copy.wait_send()


class Reduce:
    def __init__(self, ring, place, part, landing, send, recv):
        self.ring, self.part, self.landing = ring, part, landing
        self.send, self.recv = send, recv
        self.me_t = lax.axis_index("tp")
        self.goes = (ring.at(place + 1), ring.at(place - 1))
        self.share = part.shape[0] // ring.n
        self.half = part.shape[1] // 2
        self.width = self.half // CUTS
        self.sends = []

    def mine(self, way, offset, k):
        slot = self.ring.slot(offset)
        return (pl.ds(slot * self.share, self.share), pl.ds(way * self.half + k * self.width, self.width))

    def land(self, way, s, k):
        return self.landing.at[way, s, :, pl.ds(k * self.width, self.width)]

    def sem(self, way, s, k):
        return (way * (self.ring.n - 1) + s) * CUTS + k

    def arrived(self, way, s, k):
        spot, sem = self.land(way, s, k), self.sem(way, s, k)
        remote(spot, spot, self.send.at[sem], self.recv.at[sem], self.goes[way], self.me_t).wait_recv()
        return spot[...].astype(jnp.float32)

    def step(self, s):
        for k in range(CUTS):
            for way in range(2):
                rows, cols = self.mine(way, -(1 + s) if way == 0 else 1 + s, k)
                if s > 0:
                    total = self.arrived(way, s - 1, k) + self.part[rows, cols].astype(jnp.float32)
                    self.part[rows, cols] = total.astype(self.part.dtype)
                sem = self.sem(way, s, k)
                self.sends.append(remote(self.part.at[rows, cols], self.land(way, s, k), self.send.at[sem],
                                         self.recv.at[sem], self.goes[way], self.me_t))
                self.sends[-1].start()

    def last(self, store):
        for k in range(CUTS):
            for way in range(2):
                rows, cols = self.mine(way, 0, k)
                total = self.arrived(way, self.ring.n - 2, k) + self.part[rows, cols].astype(jnp.float32)
                store(cols, total)


class Gather:
    def __init__(self, ring, place, blocks, send, recv):
        self.ring, self.blocks, self.send, self.recv = ring, blocks, send, recv
        self.me_t = lax.axis_index("tp")
        self.goes = (ring.at(place + 1), ring.at(place - 1))
        self.share = blocks.shape[0] // ring.n
        self.half = blocks.shape[1] // 2
        self.far = ring.n // 2
        self.sends = []

    def spot(self, offset, k):
        slot = self.ring.slot(offset)
        return self.blocks.at[pl.ds(slot * self.share, self.share), pl.ds(k * self.half, self.half)]

    def copy(self, way, s, k):
        sign = -1 if way == 0 else 1
        sem = (way * self.far + s) * 2 + k
        return remote(self.spot(sign * s, k), self.spot(sign * (s + 1), k), self.send.at[sem],
                      self.recv.at[sem], self.goes[way], self.me_t)

    def halves(self, way, s):
        return (0, 1) if s < self.far - 1 else (way,)

    def step(self, s):
        for k in range(2):
            for way in range(2):
                if s > 0:
                    self.copy(way, s - 1, k).wait_recv()
                if k in self.halves(way, s):
                    self.sends.append(self.copy(way, s, k))
                    self.sends[-1].start()

    def last(self):
        for way in range(2):
            self.copy(way, self.far - 1, way).wait_recv()


def normalize(rows):
    return (rows * lax.rsqrt(jnp.mean(rows * rows, axis=-1, keepdims=True) + 1e-06)).astype(jnp.bfloat16)


def branch_rows(x, gu, dn, act, part, start, count):
    rows = pl.ds(start, count)
    lanes = (((1,), (1,)), ((), ()))
    for at, size in tiles(gu.shape[1], TILE):
        gate = lax.dot_general(x[rows, :], gu[0, pl.ds(at, size), :], lanes, preferred_element_type=jnp.float32)
        up = lax.dot_general(x[rows, :], gu[1, pl.ds(at, size), :], lanes, preferred_element_type=jnp.float32)
        act[:, pl.ds(at, size)] = (jax.nn.silu(gate) * up).astype(act.dtype)
    for at, size in tiles(dn.shape[1], 2 * TILE):
        part[rows, pl.ds(at, size)] = jnp.dot(
            act[...], dn[:, pl.ds(at, size)], preferred_element_type=jnp.float32
        ).astype(part.dtype)


def kernel(n_fs, n_tp, tok, gu_a, dn_a, gu_b, dn_b, gu_out_a, dn_out_a, gu_out_b, dn_out_b, done,
           x, gathered, part_a, part_b, act, mid, land_a, land_b, *sems):
    n_x = n_tp // CORES
    ring = Ring(n_fs // n_x, n_x)
    me_f, me_t = lax.axis_index("fs"), lax.axis_index("tp")
    place = ring.position(me_f // n_x, me_f % n_x)
    n, far = ring.n, ring.n // 2
    share = tok.shape[0] // n
    one = Exchange(n_fs, n_tp, gu_a, dn_a, gu_out_a, dn_out_a, sems[:11])
    two = Exchange(n_fs, n_tp, gu_b, dn_b, gu_out_b, dn_out_b, sems[11:22])
    sum_one = Reduce(ring, place, part_a, land_a, sems[22], sems[23])
    sum_two = Reduce(ring, place, part_b, land_b, sems[24], sems[25])
    spread = Gather(ring, place, gathered, sems[26], sems[27])

    barrier = pltpu.get_barrier_semaphore()

    def greet(f, t):
        pl.semaphore_signal(
            barrier, inc=1, device_id={"fs": f, "tp": t}, device_id_type=pl.DeviceIdType.MESH
        )

    holder = me_f // one.per
    is_self = holder == me_t
    for step in range(n_fs):
        f = partner(me_f, step, n_fs)
        if step == 0:
            @pl.when(jnp.logical_not(is_self))
            def _():
                greet(f, holder)
        else:
            greet(f, holder)
    for step in range(1, one.n_y):
        greet(me_f, one.peer(step) * CORES + one.my_c)
    greet(me_f, one.mate)
    greet(ring.at(place + 1), me_t)
    greet(ring.at(place - 1), me_t)
    pl.semaphore_wait(barrier, one.per * n_tp + one.n_y + 2 - jnp.where(is_self, 1, 0))

    one.start_gu()
    one.start_dn()

    @pl.loop(0, n)
    def _(j):
        sign = jnp.where(j % 2 == 0, -1, 1)
        offset = jnp.where(j < 2, j * far, sign * (j // 2))
        f = ring.at(place + offset)
        rows = tok[pl.ds(pl.multiple_of(f * share, share), share), :].astype(jnp.float32)
        x[pl.ds(pl.multiple_of(j * share, share), share), :] = normalize(rows)

    one.pass_first()
    two.start_gu()
    two.start_dn()
    one.pass_dn()
    one.pass_second()
    one.arrive_gu()
    one.arrive_dn()

    for s in range(1, far):
        branch_rows(x, gu_out_a, dn_out_a, act, part_a, 2 * s * share, 2 * share)
        sum_one.step(s - 1)
    branch_rows(x, gu_out_a, dn_out_a, act, part_a, 0, 2 * share)
    sum_one.step(far - 1)
    two.pass_first()
    for s in range(far, n - 1):
        sum_one.step(s)

    own = pl.ds(pl.multiple_of(me_f * share, share), share)

    def store_middle(cols, total):
        mid[:, cols] = (tok[own, cols].astype(jnp.float32) + 0.5 * total).astype(mid.dtype)

    sum_one.last(store_middle)
    gathered[pl.ds(0, share), :] = normalize(mid[...].astype(jnp.float32))

    spread.step(0)
    two.pass_dn()
    two.pass_second()
    two.arrive_gu()
    two.arrive_dn()
    for s in range(1, far):
        spread.step(s)
        branch_rows(gathered, gu_out_b, dn_out_b, act, part_b, 2 * s * share, 2 * share)
        sum_two.step(s - 1)
    spread.last()
    branch_rows(gathered, gu_out_b, dn_out_b, act, part_b, 0, 2 * share)
    for s in range(far - 1, n - 1):
        sum_two.step(s)

    def store_done(cols, total):
        done[:, cols] = (mid[:, cols].astype(jnp.float32) + 0.5 * total).astype(done.dtype)

    sum_two.last(store_done)

    one.drain()
    two.drain()
    for copy in sum_one.sends + spread.sends + sum_two.sends:
        copy.wait_send()


def both_half_steps(tokens, gu_a, dn_a, gu_b, dn_b):
    n_fs, n_tp = lax.axis_size("fs"), lax.axis_size("tp")
    n_y, per = n_tp // CORES, n_fs // n_tp
    count, model = tokens.shape
    share, hidden = count // n_fs, dn_a.shape[0]
    kept = tokens.dtype
    dma = pltpu.SemaphoreType.DMA
    trade = [dma((per * n_tp,)), dma((n_fs,)), dma((n_y * n_fs,)), dma((n_y * n_fs,)), dma((n_y * n_fs,)),
             dma((n_y * n_fs,)), dma, dma((n_y,)), dma((n_y,)), dma((n_y,)), dma((n_y,))]
    hops = dma((2 * (n_fs - 1) * CUTS,))
    spread = dma((2 * (n_fs // 2) * 2,))
    served = [jax.ShapeDtypeStruct((2, hidden, model), kept), jax.ShapeDtypeStruct((hidden, model), kept)]
    landing = pltpu.VMEM((2, n_fs - 1, share, model // 2), kept)
    whole = pltpu.VMEM((count, model), kept)
    return pl.pallas_call(
        functools.partial(kernel, n_fs, n_tp),
        out_shape=served + served + [jax.ShapeDtypeStruct((share, model), kept)],
        in_specs=[pl.BlockSpec(memory_space=pltpu.VMEM)] * 5,
        out_specs=[pl.BlockSpec(memory_space=pltpu.VMEM)] * 5,
        scratch_shapes=[whole, whole, whole, whole, pltpu.VMEM((2 * share, hidden), kept),
                        pltpu.VMEM((share, model), kept), landing, landing]
        + trade + trade + [hops] * 4 + [spread] * 2,
        compiler_params=pltpu.CompilerParams(
            collective_id=0, has_side_effects=True, vmem_limit_bytes=VMEM_LIMIT
        ),
        cost_estimate=pl.CostEstimate(
            flops=12 * count * model * hidden, bytes_accessed=48 * count * model, transcendentals=0
        ),
    )(tokens, gu_a, dn_a, gu_b, dn_b)


VMEM_LIMIT = 34 * 2**20


def per_device(
    prompts,
    gain_first,
    gate_first,
    up_first,
    down_first,
    gain_second,
    gate_second,
    up_second,
    down_second,
):
    def fold(gain, *matrices):
        return jnp.stack([(gain[:, None] * matrix).astype(jnp.bfloat16).T for matrix in matrices])

    tokens = prompts.reshape(-1, prompts.shape[-1])
    served_a, down_a, served_b, down_b, finished = both_half_steps(
        tokens,
        fold(gain_first, gate_first, up_first), down_first.astype(jnp.bfloat16),
        fold(gain_second, gate_second, up_second), down_second.astype(jnp.bfloat16),
    )
    return (
        served_a[0].T,
        served_a[1].T,
        down_a,
        served_b[0].T,
        served_b[1].T,
        down_b,
        finished.reshape(prompts.shape[0], -1, prompts.shape[-1]),
    )


def solution(mesh):
    in_specs = (
        P("tp", None, None),
        P("fs"),
        P("fs", "tp"),
        P("fs", "tp"),
        P("fs", "tp"),
        P("fs"),
        P("fs", "tp"),
        P("fs", "tp"),
        P("fs", "tp"),
    )
    out_specs = (
        P(None, "fs"),
        P(None, "fs"),
        P("fs", None),
        P(None, "fs"),
        P(None, "fs"),
        P("fs", None),
        P("tp", "fs", None),
    )
    return jax.shard_map(
        per_device, mesh=mesh, in_specs=in_specs, out_specs=out_specs, check_vma=False
    )
```

```python
import functools

import jax
import jax.numpy as jnp
from jax import lax
from jax.experimental import pallas as pl
from jax.experimental.pallas import tpu as pltpu
from jax.sharding import PartitionSpec as P

CORES = 2
CUTS = 2
TILE = 256


def partner(index, step, count):
    if count & (count - 1):
        return (index + step) % count
    result, bit = 0, 1
    while bit < count:
        result = result + ((index // bit + step // bit) % 2) * bit
        bit *= 2
    return result


def tiles(total, size):
    return [(start, min(size, total - start)) for start in range(0, total, size)]


class Ring:
    def __init__(self, n_z, n_x):
        self.n_z, self.n_x, self.n = n_z, n_x, n_z * n_x

    def position(self, z, x):
        if self.n_x == 1:
            return z
        row, wide = self.n_z - 1 - z, self.n_x - 1
        back = self.n_z + row * wide + jnp.where(row % 2 == 0, x - 1, self.n_x - 1 - x)
        return jnp.where(x == 0, z, back)

    def at(self, place):
        place = (place + self.n) % self.n
        if self.n_x == 1:
            return place
        wide = self.n_x - 1
        rest = place + self.n - self.n_z
        row = (rest - self.n) // wide
        col = (rest - self.n) % wide
        back = (self.n_z - 1 - row) * self.n_x + jnp.where(row % 2 == 0, 1 + col, self.n_x - 1 - col)
        return jnp.where(place < self.n_z, place * self.n_x, back)

    def slot(self, offset):
        offset = offset % self.n
        if offset == 0:
            return 0
        if 2 * offset == self.n:
            return 1
        return 2 * offset + 1 if 2 * offset < self.n else 2 * (self.n - offset)


def remote(src, dst, send, recv, f, t):
    return pltpu.make_async_remote_copy(
        src_ref=src, dst_ref=dst, send_sem=send, recv_sem=recv,
        device_id={"fs": f, "tp": t}, device_id_type=pl.DeviceIdType.MESH,
    )


class Exchange:
    def __init__(self, n_fs, n_tp, gu, dn, gu_out, dn_out, bounce, sems):
        (self.send_c, self.recv_c, self.send_n, self.send_f, self.recv_a, self.send_y, self.recv_y,
         self.send_m, self.recv_m, self.dn_local, self.dn_send_y, self.dn_recv_y, self.dn_send_m,
         self.dn_recv_m) = sems
        self.n_fs, self.n_tp, self.n_y = n_fs, n_tp, n_tp // CORES
        self.per = n_fs // n_tp
        self.gu, self.dn, self.gu_out, self.dn_out, self.bounce = gu, dn, gu_out, dn_out, bounce
        self.hidden, self.rows = gu.shape[1] // self.per, gu.shape[2]
        self.part = self.hidden // self.n_y
        self.me_f, self.me_t = lax.axis_index("fs"), lax.axis_index("tp")
        self.my_y, self.my_c = self.me_t // CORES, self.me_t % CORES
        self.mate = self.my_y * CORES + (1 - self.my_c)
        self.at_home = self.me_f // self.per // CORES == self.my_y

    def peer(self, step):
        return (self.my_y + step) % self.n_y

    def beside(self, step):
        return self.peer(step) * CORES + self.my_c

    def window(self, f, y, c):
        return self.gu_out.at[c, pl.ds(pl.multiple_of(y * self.part, 8), self.part),
                              pl.ds(pl.multiple_of(f * self.rows, 128), self.rows)]

    def own(self, kind, i, y):
        return self.gu.at[kind, pl.ds(pl.multiple_of(i * self.hidden + y * self.part, 8), self.part), :]

    def cross(self, hop, kind, i):
        sem = ((hop - 1) * 2 + kind) * self.per + i
        return remote(self.own(kind, i, self.peer(hop)), self.bounce.at[hop - 1, kind, i],
                      self.send_c.at[sem], self.recv_c.at[sem], self.me_f, self.beside(hop))

    def start_cross(self, kind):
        for hop in range(1, self.n_y):
            for i in range(self.per):
                self.cross(hop, kind, i).start()

    def deliver(self, src, send, t, kind, i, act):
        f = t * self.per + i
        dst = self.window(self.me_f, self.my_y, kind)
        recv = self.recv_a.at[self.me_f]
        here = jnp.logical_and(f == self.me_f, kind == self.my_c)

        @pl.when(jnp.logical_not(here))
        def _():
            copy = remote(src, dst, send, recv, f, self.my_y * CORES + kind)
            copy.start() if act else copy.wait_send()

        if act:
            @pl.when(here)
            def _():
                pltpu.make_async_copy(src, dst, recv).start()

    def near(self, kind, act=True):
        for i in range(self.per):
            self.deliver(self.own(kind, i, self.my_y), self.send_n.at[kind * self.per + i], self.me_t,
                         kind, i, act)

    def pass_cross(self, act=True):
        for kind in range(2):
            for hop in range(1, self.n_y):
                for i in range(self.per):
                    sem = ((hop - 1) * 2 + kind) * self.per + i
                    held = self.bounce.at[self.n_y - hop - 1, kind, i]
                    came = ((self.n_y - hop - 1) * 2 + kind) * self.per + i
                    if act:
                        remote(held, held, self.send_c.at[came], self.recv_c.at[came], self.me_f,
                               self.mate).wait_recv()
                    self.deliver(held, self.send_f.at[sem], self.beside(hop), kind, i, act)

    def columns(self, t):
        width = self.dn.shape[1]
        return self.dn_out.at[:, pl.ds(pl.multiple_of(t * width, 128), width)]

    def dn_first(self):
        mine = self.columns(self.me_t)
        copies = [remote(self.dn, mine, self.dn_send_y.at[step], self.dn_recv_y.at[self.my_y],
                         self.me_f, self.beside(step)) for step in range(1, self.n_y)]
        copies.append(remote(self.dn, mine, self.dn_send_m.at[0], self.dn_recv_m.at[self.my_y],
                             self.me_f, self.mate))
        return copies

    def start_dn(self):
        self.keep = pltpu.make_async_copy(self.dn, self.columns(self.me_t), self.dn_local)
        self.keep.start()
        for copy in self.dn_first():
            copy.start()

    def on_first(self, step):
        f = partner(self.me_f, step, self.n_fs)
        piece = self.window(f, self.my_y, self.my_c)
        slot = self.my_y * self.n_fs + f
        copies = [remote(piece, piece, self.send_y.at[(hop - 1) * self.n_fs + step], self.recv_y.at[slot],
                         self.me_f, self.beside(hop)) for hop in range(1, self.n_y)]
        copies.append(remote(piece, piece, self.send_m.at[step], self.recv_m.at[slot], self.me_f, self.mate))
        return f, piece, copies

    def pass_first(self):
        for step in range(self.n_fs):
            f, piece, copies = self.on_first(step)
            remote(piece, piece, self.send_m.at[0], self.recv_a.at[f], self.me_f, self.mate).wait_recv()
            for copy in copies:
                copy.start()

    def on_dn(self, hop):
        y = self.peer(hop)
        block = self.columns(y * CORES + self.my_c)
        return y, block, remote(block, block, self.dn_send_m.at[hop], self.dn_recv_m.at[y], self.me_f, self.mate)

    def pass_dn(self):
        for hop in range(1, self.n_y):
            y, block, copy = self.on_dn(hop)
            remote(block, block, self.dn_send_m.at[hop], self.dn_recv_y.at[y], self.me_f, self.mate).wait_recv()
            copy.start()

    def on_second(self, step, hop):
        f, y = partner(self.me_f, step, self.n_fs), self.peer(hop)
        piece = self.window(f, y, self.my_c)
        slot = y * self.n_fs + f
        send = self.send_m.at[hop * self.n_fs + step]
        return slot, piece, send, remote(piece, piece, send, self.recv_m.at[slot], self.me_f, self.mate)

    def pass_second(self):
        for step in range(self.n_fs):
            for hop in range(1, self.n_y):
                slot, piece, send, copy = self.on_second(step, hop)
                remote(piece, piece, send, self.recv_y.at[slot], self.me_f, self.mate).wait_recv()
                copy.start()

    def arrive_gu(self):
        for hop in range(self.n_y):
            y = self.peer(hop)
            for step in range(self.n_fs):
                f = partner(self.me_f, step, self.n_fs)
                piece = self.window(f, y, 1 - self.my_c)
                remote(piece, piece, self.send_m.at[0], self.recv_m.at[y * self.n_fs + f],
                       self.me_f, self.mate).wait_recv()

    def arrive_dn(self):
        for hop in range(self.n_y):
            y = self.peer(hop)
            block = self.columns(y * CORES + (1 - self.my_c))
            remote(block, block, self.dn_send_m.at[0], self.dn_recv_m.at[y], self.me_f, self.mate).wait_recv()
        self.keep.wait()

    def drain(self):
        for kind in range(2):
            for hop in range(1, self.n_y):
                for i in range(self.per):
                    self.cross(hop, kind, i).wait_send()
            self.near(kind, False)
        self.pass_cross(False)
        copies = self.dn_first() + [self.on_dn(hop)[2] for hop in range(1, self.n_y)]
        for step in range(self.n_fs):
            copies += self.on_first(step)[2] + [self.on_second(step, hop)[3] for hop in range(1, self.n_y)]
        for copy in copies:
            copy.wait_send()


class Reduce:
    def __init__(self, ring, place, part, landing, send, recv):
        self.ring, self.part, self.landing = ring, part, landing
        self.send, self.recv = send, recv
        self.me_t = lax.axis_index("tp")
        self.goes = (ring.at(place + 1), ring.at(place - 1))
        self.share = part.shape[0] // ring.n
        self.half = part.shape[1] // 2
        self.width = self.half // CUTS
        self.sends = []

    def mine(self, way, offset, k):
        slot = self.ring.slot(offset)
        return (pl.ds(slot * self.share, self.share), pl.ds(way * self.half + k * self.width, self.width))

    def land(self, way, s, k):
        return self.landing.at[way, s, :, pl.ds(k * self.width, self.width)]

    def sem(self, way, s, k):
        return (way * (self.ring.n - 1) + s) * CUTS + k

    def arrived(self, way, s, k):
        spot, sem = self.land(way, s, k), self.sem(way, s, k)
        remote(spot, spot, self.send.at[sem], self.recv.at[sem], self.goes[way], self.me_t).wait_recv()
        return spot[...].astype(jnp.float32)

    def step(self, s):
        for k in range(CUTS):
            for way in range(2):
                rows, cols = self.mine(way, -(1 + s) if way == 0 else 1 + s, k)
                if s > 0:
                    total = self.arrived(way, s - 1, k) + self.part[rows, cols].astype(jnp.float32)
                    self.part[rows, cols] = total.astype(self.part.dtype)
                sem = self.sem(way, s, k)
                self.sends.append(remote(self.part.at[rows, cols], self.land(way, s, k), self.send.at[sem],
                                         self.recv.at[sem], self.goes[way], self.me_t))
                self.sends[-1].start()

    def last(self, store):
        for k in range(CUTS):
            for way in range(2):
                rows, cols = self.mine(way, 0, k)
                total = self.arrived(way, self.ring.n - 2, k) + self.part[rows, cols].astype(jnp.float32)
                store(cols, total)


class Gather:
    def __init__(self, ring, place, blocks, send, recv):
        self.ring, self.blocks, self.send, self.recv = ring, blocks, send, recv
        self.me_t = lax.axis_index("tp")
        self.goes = (ring.at(place + 1), ring.at(place - 1))
        self.share = blocks.shape[0] // ring.n
        self.half = blocks.shape[1] // 2
        self.far = ring.n // 2
        self.sends = []

    def spot(self, offset, k):
        slot = self.ring.slot(offset)
        return self.blocks.at[pl.ds(slot * self.share, self.share), pl.ds(k * self.half, self.half)]

    def copy(self, way, s, k):
        sign = -1 if way == 0 else 1
        sem = (way * self.far + s) * 2 + k
        return remote(self.spot(sign * s, k), self.spot(sign * (s + 1), k), self.send.at[sem],
                      self.recv.at[sem], self.goes[way], self.me_t)

    def halves(self, way, s):
        return (0, 1) if s < self.far - 1 else (way,)

    def step(self, s):
        for k in range(2):
            for way in range(2):
                if s > 0:
                    self.copy(way, s - 1, k).wait_recv()
                if k in self.halves(way, s):
                    self.sends.append(self.copy(way, s, k))
                    self.sends[-1].start()

    def last(self):
        for way in range(2):
            self.copy(way, self.far - 1, way).wait_recv()


def normalize(rows):
    return (rows * lax.rsqrt(jnp.mean(rows * rows, axis=-1, keepdims=True) + 1e-06)).astype(jnp.bfloat16)


def branch_rows(x, gu, dn, act, part, start, count):
    rows = pl.ds(start, count)
    lanes = (((1,), (1,)), ((), ()))
    for at, size in tiles(gu.shape[1], TILE):
        gate = lax.dot_general(x[rows, :], gu[0, pl.ds(at, size), :], lanes, preferred_element_type=jnp.float32)
        up = lax.dot_general(x[rows, :], gu[1, pl.ds(at, size), :], lanes, preferred_element_type=jnp.float32)
        act[:, pl.ds(at, size)] = (jax.nn.silu(gate) * up).astype(act.dtype)
    for at, size in tiles(dn.shape[1], 2 * TILE):
        part[rows, pl.ds(at, size)] = jnp.dot(
            act[...], dn[:, pl.ds(at, size)], preferred_element_type=jnp.float32
        ).astype(part.dtype)


def fold(staged, gain, kind, gu):
    count = staged.shape[2]

    def turn(cols, size):
        gu[kind, pl.ds(cols, size), :] = (staged[kind, :, pl.ds(cols, size)].T * gain[...]).astype(gu.dtype)

    @pl.loop(0, count // LANES)
    def _(j):
        turn(pl.multiple_of(j * LANES, LANES), LANES)

    if count % LANES:
        turn(count - count % LANES, count % LANES)


def kernel(n_fs, n_tp, tok, gain_a, gain_b, gate_a, up_a, down_a, gate_b, up_b, down_b,
           gu_out_a, dn_out_a, gu_out_b, dn_out_b, done,
           staged, staged_dn, gu_a, gu_b, dn_a, dn_b, bounce_a, bounce_b,
           x, part, act, mid, landing, load_sems, *sems):
    n_x = n_tp // CORES
    ring = Ring(n_fs // n_x, n_x)
    me_f, me_t = lax.axis_index("fs"), lax.axis_index("tp")
    place = ring.position(me_f // n_x, me_f % n_x)
    n, far = ring.n, ring.n // 2
    share = tok.shape[0] // n
    each = TRADE_SEMS
    one = Exchange(n_fs, n_tp, gu_a, dn_a, gu_out_a, dn_out_a, bounce_a, sems[:each])
    two = Exchange(n_fs, n_tp, gu_b, dn_b, gu_out_b, dn_out_b, bounce_b, sems[each:2 * each])
    rest = sems[2 * each:]
    sum_one = Reduce(ring, place, part, landing, rest[0], rest[1])
    sum_two = Reduce(ring, place, part, landing, rest[2], rest[3])
    spread = Gather(ring, place, x, rest[4], rest[5])

    def load(step, gate, up, down):
        return [pltpu.make_async_copy(src, dst, load_sems.at[3 * step + i])
                for i, (src, dst) in enumerate(((gate, staged.at[0]), (up, staged.at[1]), (down, staged_dn)))]

    loads = load(0, gate_a, up_a, down_a)
    for copy in loads:
        copy.start()

    barrier = pltpu.get_barrier_semaphore()

    def greet(f, t):
        pl.semaphore_signal(
            barrier, inc=1, device_id={"fs": f, "tp": t}, device_id_type=pl.DeviceIdType.MESH
        )

    core = me_f // one.per % CORES
    is_self = core == one.my_c
    for step in range(n_fs):
        f = partner(me_f, step, n_fs)
        if step == 0:
            @pl.when(jnp.logical_not(is_self))
            def _():
                greet(f, one.my_y * CORES + core)
        else:
            greet(f, one.my_y * CORES + core)
    for step in range(1, one.n_y):
        greet(me_f, one.beside(step))
    greet(me_f, one.mate)
    greet(ring.at(place + 1), me_t)
    greet(ring.at(place - 1), me_t)
    pl.semaphore_wait(barrier, n_fs + one.n_y + 2 - jnp.where(is_self, 1, 0))

    for kind in range(2):
        loads[kind].wait()
        fold(staged, gain_a, kind, gu_a)
        one.start_cross(kind)
        one.near(kind)
    loads[2].wait()
    dn_a[...] = staged_dn[...].astype(dn_a.dtype)
    one.start_dn()
    loads = load(1, gate_b, up_b, down_b)
    for copy in loads:
        copy.start()

    @pl.loop(0, n)
    def _(j):
        sign = jnp.where(j % 2 == 0, -1, 1)
        offset = jnp.where(j < 2, j * far, sign * (j // 2))
        f = ring.at(place + offset)
        rows = tok[pl.ds(pl.multiple_of(f * share, share), share), :].astype(jnp.float32)
        x[pl.ds(pl.multiple_of(j * share, share), share), :] = normalize(rows)

    one.pass_cross()
    for kind in range(2):
        loads[kind].wait()
        fold(staged, gain_b, kind, gu_b)
        two.near(kind)
    loads[2].wait()
    dn_b[...] = staged_dn[...].astype(dn_b.dtype)

    one.pass_first()
    two.start_cross(0)
    two.start_cross(1)
    one.pass_dn()
    one.pass_second()
    one.arrive_gu()
    one.arrive_dn()

    @pl.when(two.at_home)
    def _():
        two.pass_first()

    two.start_dn()

    for s in range(1, far):
        branch_rows(x, gu_out_a, dn_out_a, act, part, 2 * s * share, 2 * share)
        sum_one.step(s - 1)
        if s == 1:
            two.pass_cross()
    branch_rows(x, gu_out_a, dn_out_a, act, part, 0, 2 * share)
    sum_one.step(far - 1)

    @pl.when(jnp.logical_not(two.at_home))
    def _():
        two.pass_first()

    for s in range(far, n - 1):
        sum_one.step(s)

    own = pl.ds(pl.multiple_of(me_f * share, share), share)

    def store_middle(cols, total):
        mid[:, cols] = (tok[own, cols].astype(jnp.float32) + 0.5 * total).astype(mid.dtype)

    sum_one.last(store_middle)
    x[pl.ds(0, share), :] = normalize(mid[...].astype(jnp.float32))

    spread.step(0)
    two.pass_dn()
    for copy in sum_one.sends:
        copy.wait_send()
    spread.step(1)
    two.pass_second()
    two.arrive_gu()
    two.arrive_dn()
    for s in range(1, far):
        if s > 1:
            spread.step(s)
        branch_rows(x, gu_out_b, dn_out_b, act, part, 2 * s * share, 2 * share)
        sum_two.step(s - 1)
    spread.last()
    branch_rows(x, gu_out_b, dn_out_b, act, part, 0, 2 * share)
    for s in range(far - 1, n - 1):
        sum_two.step(s)

    def store_done(cols, total):
        done[:, cols] = (mid[:, cols].astype(jnp.float32) + 0.5 * total).astype(done.dtype)

    sum_two.last(store_done)

    one.drain()
    two.drain()
    for copy in spread.sends + sum_two.sends:
        copy.wait_send()


TRADE_SEMS = 14
LANES = 128
VMEM_LIMIT = 32 * 2**20


def stay(array):
    return pltpu.with_memory_space_constraint(array, pltpu.HBM)


def both_half_steps(tokens, gains, first, second):
    n_fs, n_tp = lax.axis_size("fs"), lax.axis_size("tp")
    n_y, per = n_tp // CORES, n_fs // n_tp
    count, model = tokens.shape
    rows, wide = first[0].shape
    share, hidden = count // n_fs, wide // per
    kept = tokens.dtype
    dma = pltpu.SemaphoreType.DMA
    hop, every = dma(((n_y - 1) * 2 * per,)), dma((n_y * n_fs,))
    trade = [hop, hop, dma((2 * per,)), hop, dma((n_fs,)), every, every, every, every, dma, dma((n_y,)),
             dma((n_y,)), dma((n_y,)), dma((n_y,))]
    hops = dma((2 * (n_fs - 1) * CUTS,))
    spread = dma((2 * (n_fs // 2) * 2,))
    served = [jax.ShapeDtypeStruct((2, hidden, model), kept), jax.ShapeDtypeStruct((hidden, model), kept)]
    vmem = pltpu.VMEM
    folded, down = vmem((2, wide, rows), kept), vmem(first[2].shape, kept)
    bounce = vmem((n_y - 1, 2, per, hidden // n_y, rows), kept)
    return pl.pallas_call(
        functools.partial(kernel, n_fs, n_tp),
        out_shape=served + served + [jax.ShapeDtypeStruct((share, model), kept)],
        in_specs=[pl.BlockSpec(memory_space=vmem)] * 3 + [pl.BlockSpec(memory_space=pltpu.HBM)] * 6,
        out_specs=[pl.BlockSpec(memory_space=vmem)] * 5,
        scratch_shapes=[
            vmem((2, rows, wide), first[0].dtype), vmem(first[2].shape, first[2].dtype),
            folded, folded, down, down, bounce, bounce,
            vmem((count, model), kept), vmem((count, model), kept), vmem((2 * share, hidden), kept),
            vmem((share, model), kept), vmem((2, n_fs - 1, share, model // 2), kept), dma((6,)),
        ] + trade + trade + [hops] * 4 + [spread] * 2,
        compiler_params=pltpu.CompilerParams(
            collective_id=0, has_side_effects=True, vmem_limit_bytes=VMEM_LIMIT
        ),
        cost_estimate=pl.CostEstimate(
            flops=12 * count * model * hidden, bytes_accessed=48 * count * model, transcendentals=0
        ),
    )(tokens, *gains, *map(stay, first + second))


def place_kernel(gu_a, dn_a, gu_b, dn_b, done, *refs):
    outs, sems = refs[:-1], refs[-1]
    sources = (gu_a.at[0], gu_a.at[1], dn_a, gu_b.at[0], gu_b.at[1], dn_b, done)
    copies = [pltpu.make_async_copy(src, dst, sems.at[i]) for i, (src, dst) in enumerate(zip(sources, outs))]
    for copy in copies:
        copy.start()
    for copy in copies:
        copy.wait()


def place_results(gu_a, dn_a, gu_b, dn_b, done):
    block = jax.ShapeDtypeStruct(dn_a.shape, dn_a.dtype)
    outs = [block] * 6 + [jax.ShapeDtypeStruct(done.shape, done.dtype)]
    return pl.pallas_call(
        place_kernel,
        out_shape=outs,
        in_specs=[pl.BlockSpec(memory_space=pltpu.VMEM)] * 5,
        out_specs=[pl.BlockSpec(memory_space=pltpu.HBM)] * 7,
        scratch_shapes=[pltpu.SemaphoreType.DMA((7,))],
        compiler_params=pltpu.CompilerParams(vmem_limit_bytes=2**20),
    )(gu_a, dn_a, gu_b, dn_b, done)


def per_device(
    prompts,
    gain_first,
    gate_first,
    up_first,
    down_first,
    gain_second,
    gate_second,
    up_second,
    down_second,
):
    tokens = prompts.reshape(-1, prompts.shape[-1])
    gate_a, up_a, down_a, gate_b, up_b, down_b, finished = place_results(*both_half_steps(
        tokens, (gain_first[None], gain_second[None]),
        (gate_first, up_first, down_first), (gate_second, up_second, down_second),
    ))
    return (
        gate_a.T,
        up_a.T,
        down_a,
        gate_b.T,
        up_b.T,
        down_b,
        finished.reshape(prompts.shape[0], -1, prompts.shape[-1]),
    )


def solution(mesh):
    in_specs = (
        P("tp", None, None),
        P("fs"),
        P("fs", "tp"),
        P("fs", "tp"),
        P("fs", "tp"),
        P("fs"),
        P("fs", "tp"),
        P("fs", "tp"),
        P("fs", "tp"),
    )
    out_specs = (
        P(None, "fs"),
        P(None, "fs"),
        P("fs", None),
        P(None, "fs"),
        P(None, "fs"),
        P("fs", None),
        P("tp", "fs", None),
    )
    return jax.shard_map(
        per_device, mesh=mesh, in_specs=in_specs, out_specs=out_specs, check_vma=False
    )
```

```python
import functools

import jax
import jax.numpy as jnp
from jax import lax
from jax.experimental import pallas as pl
from jax.experimental.pallas import tpu as pltpu
from jax.sharding import PartitionSpec as P

CORES = 2
CUTS = 2
TILE = 256


def partner(index, step, count):
    if count & (count - 1):
        return (index + step) % count
    result, bit = 0, 1
    while bit < count:
        result = result + ((index // bit + step // bit) % 2) * bit
        bit *= 2
    return result


def tiles(total, size):
    return [(start, min(size, total - start)) for start in range(0, total, size)]


class Ring:
    def __init__(self, n_z, n_x):
        self.n_z, self.n_x, self.n = n_z, n_x, n_z * n_x

    def position(self, z, x):
        if self.n_x == 1:
            return z
        row, wide = self.n_z - 1 - z, self.n_x - 1
        back = self.n_z + row * wide + jnp.where(row % 2 == 0, x - 1, self.n_x - 1 - x)
        return jnp.where(x == 0, z, back)

    def at(self, place):
        place = (place + self.n) % self.n
        if self.n_x == 1:
            return place
        wide = self.n_x - 1
        rest = place + self.n - self.n_z
        row = (rest - self.n) // wide
        col = (rest - self.n) % wide
        back = (self.n_z - 1 - row) * self.n_x + jnp.where(row % 2 == 0, 1 + col, self.n_x - 1 - col)
        return jnp.where(place < self.n_z, place * self.n_x, back)

    def slot(self, offset):
        offset = offset % self.n
        if offset == 0:
            return 0
        if 2 * offset == self.n:
            return 1
        return 2 * offset + 1 if 2 * offset < self.n else 2 * (self.n - offset)


def remote(src, dst, send, recv, f, t):
    return pltpu.make_async_remote_copy(
        src_ref=src, dst_ref=dst, send_sem=send, recv_sem=recv,
        device_id={"fs": f, "tp": t}, device_id_type=pl.DeviceIdType.MESH,
    )


class Exchange:
    def __init__(self, n_fs, n_tp, gu, dn, gu_out, dn_out, bounce, sems):
        (self.send_c, self.recv_c, self.send_n, self.send_f, self.recv_a, self.send_y, self.recv_y,
         self.send_m, self.recv_m, self.dn_local, self.dn_send_y, self.dn_recv_y, self.dn_send_m,
         self.dn_recv_m) = sems
        self.n_fs, self.n_tp, self.n_y = n_fs, n_tp, n_tp // CORES
        self.per = n_fs // n_tp
        self.gu, self.dn, self.gu_out, self.dn_out, self.bounce = gu, dn, gu_out, dn_out, bounce
        self.hidden, self.rows = gu.shape[1] // self.per, gu.shape[2]
        self.part = self.hidden // self.n_y
        self.me_f, self.me_t = lax.axis_index("fs"), lax.axis_index("tp")
        self.my_y, self.my_c = self.me_t // CORES, self.me_t % CORES
        self.mate = self.my_y * CORES + (1 - self.my_c)
        self.at_home = self.me_f // self.per // CORES == self.my_y

    def peer(self, step):
        return (self.my_y + step) % self.n_y

    def beside(self, step):
        return self.peer(step) * CORES + self.my_c

    def window(self, f, y, c):
        return self.gu_out.at[c, pl.ds(pl.multiple_of(y * self.part, 8), self.part),
                              pl.ds(pl.multiple_of(f * self.rows, 128), self.rows)]

    def own(self, kind, i, y):
        return self.gu.at[kind, pl.ds(pl.multiple_of(i * self.hidden + y * self.part, 8), self.part), :]

    def cross(self, hop, kind, i):
        sem = ((hop - 1) * 2 + kind) * self.per + i
        return remote(self.own(kind, i, self.peer(hop)), self.bounce.at[hop - 1, kind, i],
                      self.send_c.at[sem], self.recv_c.at[sem], self.me_f, self.beside(hop))

    def start_cross(self, kind):
        for hop in range(1, self.n_y):
            for i in range(self.per):
                self.cross(hop, kind, i).start()

    def deliver(self, src, send, t, kind, i, act):
        f = t * self.per + i
        dst = self.window(self.me_f, self.my_y, kind)
        recv = self.recv_a.at[self.me_f]
        here = jnp.logical_and(f == self.me_f, kind == self.my_c)

        @pl.when(jnp.logical_not(here))
        def _():
            copy = remote(src, dst, send, recv, f, self.my_y * CORES + kind)
            copy.start() if act else copy.wait_send()

        if act:
            @pl.when(here)
            def _():
                pltpu.make_async_copy(src, dst, recv).start()

    def near(self, kind, act=True):
        for i in range(self.per):
            self.deliver(self.own(kind, i, self.my_y), self.send_n.at[kind * self.per + i], self.me_t,
                         kind, i, act)

    def pass_cross(self, act=True):
        for kind in range(2):
            for hop in range(1, self.n_y):
                for i in range(self.per):
                    sem = ((hop - 1) * 2 + kind) * self.per + i
                    held = self.bounce.at[self.n_y - hop - 1, kind, i]
                    came = ((self.n_y - hop - 1) * 2 + kind) * self.per + i
                    if act:
                        remote(held, held, self.send_c.at[came], self.recv_c.at[came], self.me_f,
                               self.mate).wait_recv()
                    self.deliver(held, self.send_f.at[sem], self.beside(hop), kind, i, act)

    def columns(self, t):
        width = self.dn.shape[1]
        return self.dn_out.at[:, pl.ds(pl.multiple_of(t * width, 128), width)]

    def dn_first(self):
        mine = self.columns(self.me_t)
        copies = [remote(self.dn, mine, self.dn_send_y.at[step], self.dn_recv_y.at[self.my_y],
                         self.me_f, self.beside(step)) for step in range(1, self.n_y)]
        copies.append(remote(self.dn, mine, self.dn_send_m.at[0], self.dn_recv_m.at[self.my_y],
                             self.me_f, self.mate))
        return copies

    def start_dn(self):
        self.keep = pltpu.make_async_copy(self.dn, self.columns(self.me_t), self.dn_local)
        self.keep.start()
        for copy in self.dn_first():
            copy.start()

    def on_first(self, step):
        f = partner(self.me_f, step, self.n_fs)
        piece = self.window(f, self.my_y, self.my_c)
        slot = self.my_y * self.n_fs + f
        copies = [remote(piece, piece, self.send_y.at[(hop - 1) * self.n_fs + step], self.recv_y.at[slot],
                         self.me_f, self.beside(hop)) for hop in range(1, self.n_y)]
        copies.append(remote(piece, piece, self.send_m.at[step], self.recv_m.at[slot], self.me_f, self.mate))
        return f, piece, copies

    def pass_first(self, steps):
        for step in steps:
            f, piece, copies = self.on_first(step)
            remote(piece, piece, self.send_m.at[0], self.recv_a.at[f], self.me_f, self.mate).wait_recv()
            for copy in copies:
                copy.start()

    def on_dn(self, hop):
        y = self.peer(hop)
        block = self.columns(y * CORES + self.my_c)
        return y, block, remote(block, block, self.dn_send_m.at[hop], self.dn_recv_m.at[y], self.me_f, self.mate)

    def pass_dn(self):
        for hop in range(1, self.n_y):
            y, block, copy = self.on_dn(hop)
            remote(block, block, self.dn_send_m.at[hop], self.dn_recv_y.at[y], self.me_f, self.mate).wait_recv()
            copy.start()

    def on_second(self, step, hop):
        f, y = partner(self.me_f, step, self.n_fs), self.peer(hop)
        piece = self.window(f, y, self.my_c)
        slot = y * self.n_fs + f
        send = self.send_m.at[hop * self.n_fs + step]
        return slot, piece, send, remote(piece, piece, send, self.recv_m.at[slot], self.me_f, self.mate)

    def pass_second(self):
        for step in range(self.n_fs):
            for hop in range(1, self.n_y):
                slot, piece, send, copy = self.on_second(step, hop)
                remote(piece, piece, send, self.recv_y.at[slot], self.me_f, self.mate).wait_recv()
                copy.start()

    def arrive_gu(self):
        for hop in range(self.n_y):
            y = self.peer(hop)
            for step in range(self.n_fs):
                f = partner(self.me_f, step, self.n_fs)
                piece = self.window(f, y, 1 - self.my_c)
                remote(piece, piece, self.send_m.at[0], self.recv_m.at[y * self.n_fs + f],
                       self.me_f, self.mate).wait_recv()

    def arrive_dn(self):
        for hop in range(self.n_y):
            y = self.peer(hop)
            block = self.columns(y * CORES + (1 - self.my_c))
            remote(block, block, self.dn_send_m.at[0], self.dn_recv_m.at[y], self.me_f, self.mate).wait_recv()
        self.keep.wait()

    def drain(self):
        for kind in range(2):
            for hop in range(1, self.n_y):
                for i in range(self.per):
                    self.cross(hop, kind, i).wait_send()
            self.near(kind, False)
        self.pass_cross(False)
        copies = self.dn_first() + [self.on_dn(hop)[2] for hop in range(1, self.n_y)]
        for step in range(self.n_fs):
            copies += self.on_first(step)[2] + [self.on_second(step, hop)[3] for hop in range(1, self.n_y)]
        for copy in copies:
            copy.wait_send()


class Reduce:
    def __init__(self, ring, place, part, landing, send, recv):
        self.ring, self.part, self.landing = ring, part, landing
        self.send, self.recv = send, recv
        self.me_t = lax.axis_index("tp")
        self.goes = (ring.at(place + 1), ring.at(place - 1))
        self.share = part.shape[0] // ring.n
        self.half = part.shape[1] // 2
        self.width = self.half // CUTS
        self.sends = []

    def mine(self, way, offset, k):
        slot = self.ring.slot(offset)
        return (pl.ds(slot * self.share, self.share), pl.ds(way * self.half + k * self.width, self.width))

    def land(self, way, s, k):
        return self.landing.at[way, s, :, pl.ds(k * self.width, self.width)]

    def sem(self, way, s, k):
        return (way * (self.ring.n - 1) + s) * CUTS + k

    def arrived(self, way, s, k):
        spot, sem = self.land(way, s, k), self.sem(way, s, k)
        remote(spot, spot, self.send.at[sem], self.recv.at[sem], self.goes[way], self.me_t).wait_recv()
        return spot[...].astype(jnp.float32)

    def step(self, s):
        for k in range(CUTS):
            for way in range(2):
                rows, cols = self.mine(way, -(1 + s) if way == 0 else 1 + s, k)
                if s > 0:
                    total = self.arrived(way, s - 1, k) + self.part[rows, cols].astype(jnp.float32)
                    self.part[rows, cols] = total.astype(self.part.dtype)
                sem = self.sem(way, s, k)
                self.sends.append(remote(self.part.at[rows, cols], self.land(way, s, k), self.send.at[sem],
                                         self.recv.at[sem], self.goes[way], self.me_t))
                self.sends[-1].start()

    def last(self, store):
        for k in range(CUTS):
            for way in range(2):
                rows, cols = self.mine(way, 0, k)
                total = self.arrived(way, self.ring.n - 2, k) + self.part[rows, cols].astype(jnp.float32)
                store(cols, total)


class Gather:
    def __init__(self, ring, place, blocks, send, recv):
        self.ring, self.blocks, self.send, self.recv = ring, blocks, send, recv
        self.me_t = lax.axis_index("tp")
        self.goes = (ring.at(place + 1), ring.at(place - 1))
        self.share = blocks.shape[0] // ring.n
        self.half = blocks.shape[1] // 2
        self.far = ring.n // 2
        self.sends = []

    def spot(self, offset, k):
        slot = self.ring.slot(offset)
        return self.blocks.at[pl.ds(slot * self.share, self.share), pl.ds(k * self.half, self.half)]

    def copy(self, way, s, k):
        sign = -1 if way == 0 else 1
        sem = (way * self.far + s) * 2 + k
        return remote(self.spot(sign * s, k), self.spot(sign * (s + 1), k), self.send.at[sem],
                      self.recv.at[sem], self.goes[way], self.me_t)

    def halves(self, way, s):
        return (0, 1) if s < self.far - 1 else (way,)

    def step(self, s):
        for k in range(2):
            for way in range(2):
                if s > 0:
                    self.copy(way, s - 1, k).wait_recv()
                if k in self.halves(way, s):
                    self.sends.append(self.copy(way, s, k))
                    self.sends[-1].start()

    def last(self):
        for way in range(2):
            self.copy(way, self.far - 1, way).wait_recv()


def normalize(rows):
    return (rows * lax.rsqrt(jnp.mean(rows * rows, axis=-1, keepdims=True) + 1e-06)).astype(jnp.bfloat16)


def active_rows(x, gu, act, start, count):
    rows = pl.ds(start, count)
    lanes = (((1,), (1,)), ((), ()))
    for at, size in tiles(gu.shape[1], TILE):
        gate = lax.dot_general(x[rows, :], gu[0, pl.ds(at, size), :], lanes, preferred_element_type=jnp.float32)
        up = lax.dot_general(x[rows, :], gu[1, pl.ds(at, size), :], lanes, preferred_element_type=jnp.float32)
        act[rows, pl.ds(at, size)] = (jax.nn.silu(gate) * up).astype(act.dtype)


def down_rows(act, dn, part, start, count):
    rows = pl.ds(start, count)
    for at, size in tiles(dn.shape[1], 2 * TILE):
        part[rows, pl.ds(at, size)] = jnp.dot(
            act[rows, :], dn[:, pl.ds(at, size)], preferred_element_type=jnp.float32
        ).astype(part.dtype)


def fold(staged, gain, kind, gu):
    count = staged.shape[2]

    def turn(cols, size):
        gu[kind, pl.ds(cols, size), :] = (staged[kind, :, pl.ds(cols, size)].T * gain[...]).astype(gu.dtype)

    @pl.loop(0, count // LANES)
    def _(j):
        turn(pl.multiple_of(j * LANES, LANES), LANES)

    if count % LANES:
        turn(count - count % LANES, count % LANES)


def kernel(n_fs, n_tp, tok, gain_a, gain_b, gate_a, up_a, down_a, gate_b, up_b, down_b,
           gu_out_a, dn_out_a, gu_out_b, dn_out_b, done,
           staged, staged_dn, gu_a, gu_b, dn_a, dn_b, bounce_a, bounce_b,
           x, part, act, mid, landing, load_sems, *sems):
    n_x = n_tp // CORES
    ring = Ring(n_fs // n_x, n_x)
    me_f, me_t = lax.axis_index("fs"), lax.axis_index("tp")
    place = ring.position(me_f // n_x, me_f % n_x)
    n, far = ring.n, ring.n // 2
    share = tok.shape[0] // n
    each = TRADE_SEMS
    one = Exchange(n_fs, n_tp, gu_a, dn_a, gu_out_a, dn_out_a, bounce_a, sems[:each])
    two = Exchange(n_fs, n_tp, gu_b, dn_b, gu_out_b, dn_out_b, bounce_b, sems[each:2 * each])
    rest = sems[2 * each:]
    sum_one = Reduce(ring, place, part, landing, rest[0], rest[1])
    sum_two = Reduce(ring, place, part, landing, rest[2], rest[3])
    spread = Gather(ring, place, x, rest[4], rest[5])

    def load(step, gate, up, down):
        return [pltpu.make_async_copy(src, dst, load_sems.at[3 * step + i])
                for i, (src, dst) in enumerate(((gate, staged.at[0]), (up, staged.at[1]), (down, staged_dn)))]

    loads = load(0, gate_a, up_a, down_a)
    for copy in loads:
        copy.start()

    barrier = pltpu.get_barrier_semaphore()

    def greet(f, t):
        pl.semaphore_signal(
            barrier, inc=1, device_id={"fs": f, "tp": t}, device_id_type=pl.DeviceIdType.MESH
        )

    core = me_f // one.per % CORES
    is_self = core == one.my_c
    for step in range(n_fs):
        f = partner(me_f, step, n_fs)
        if step == 0:
            @pl.when(jnp.logical_not(is_self))
            def _():
                greet(f, one.my_y * CORES + core)
        else:
            greet(f, one.my_y * CORES + core)
    for step in range(1, one.n_y):
        greet(me_f, one.beside(step))
    greet(me_f, one.mate)
    greet(ring.at(place + 1), me_t)
    greet(ring.at(place - 1), me_t)
    pl.semaphore_wait(barrier, n_fs + one.n_y + 2 - jnp.where(is_self, 1, 0))

    for kind in range(2):
        loads[kind].wait()
        fold(staged, gain_a, kind, gu_a)
        one.start_cross(kind)
        one.near(kind)
    loads[2].wait()
    dn_a[...] = staged_dn[...].astype(dn_a.dtype)
    loads = load(1, gate_b, up_b, down_b)
    for copy in loads:
        copy.start()

    @pl.loop(0, n)
    def _(j):
        sign = jnp.where(j % 2 == 0, -1, 1)
        offset = jnp.where(j < 2, j * far, sign * (j // 2))
        f = ring.at(place + offset)
        rows = tok[pl.ds(pl.multiple_of(f * share, share), share), :].astype(jnp.float32)
        x[pl.ds(pl.multiple_of(j * share, share), share), :] = normalize(rows)

    for kind in range(2):
        loads[kind].wait()
        fold(staged, gain_b, kind, gu_b)
        two.start_cross(kind)
        two.near(kind)
    loads[2].wait()
    dn_b[...] = staged_dn[...].astype(dn_b.dtype)

    one.pass_cross()
    one.pass_first(range(n_fs // 2))
    two.pass_cross()
    one.pass_first(range(n_fs // 2, n_fs))
    one.start_dn()
    one.pass_second()
    one.arrive_gu()

    @pl.loop(0, far)
    def _(j):
        active_rows(x, gu_out_a, act, pl.multiple_of(j * 2 * share, 2 * share), 2 * share)

    two.pass_first(range(n_fs))
    two.start_dn()
    one.pass_dn()
    one.arrive_dn()
    for s in range(1, far):
        down_rows(act, dn_out_a, part, 2 * s * share, 2 * share)
        sum_one.step(s - 1)
    down_rows(act, dn_out_a, part, 0, 2 * share)
    for s in range(far - 1, n - 1):
        sum_one.step(s)

    own = pl.ds(pl.multiple_of(me_f * share, share), share)

    def store_middle(cols, total):
        mid[:, cols] = (tok[own, cols].astype(jnp.float32) + 0.5 * total).astype(mid.dtype)

    sum_one.last(store_middle)
    x[pl.ds(0, share), :] = normalize(mid[...].astype(jnp.float32))

    spread.step(0)
    two.pass_dn()
    for copy in sum_one.sends:
        copy.wait_send()
    spread.step(1)
    two.pass_second()
    two.arrive_gu()
    two.arrive_dn()
    for s in range(1, far):
        if s > 1:
            spread.step(s)
        active_rows(x, gu_out_b, act, 2 * s * share, 2 * share)
        down_rows(act, dn_out_b, part, 2 * s * share, 2 * share)
        sum_two.step(s - 1)
    spread.last()
    active_rows(x, gu_out_b, act, 0, 2 * share)
    down_rows(act, dn_out_b, part, 0, 2 * share)
    for s in range(far - 1, n - 1):
        sum_two.step(s)

    def store_done(cols, total):
        done[:, cols] = (mid[:, cols].astype(jnp.float32) + 0.5 * total).astype(done.dtype)

    sum_two.last(store_done)

    one.drain()
    two.drain()
    for copy in spread.sends + sum_two.sends:
        copy.wait_send()


TRADE_SEMS = 14
LANES = 128
VMEM_LIMIT = 32 * 2**20


def stay(array):
    return pltpu.with_memory_space_constraint(array, pltpu.HBM)


def both_half_steps(tokens, gains, first, second):
    n_fs, n_tp = lax.axis_size("fs"), lax.axis_size("tp")
    n_y, per = n_tp // CORES, n_fs // n_tp
    count, model = tokens.shape
    rows, wide = first[0].shape
    share, hidden = count // n_fs, wide // per
    kept = tokens.dtype
    dma = pltpu.SemaphoreType.DMA
    hop, every = dma(((n_y - 1) * 2 * per,)), dma((n_y * n_fs,))
    trade = [hop, hop, dma((2 * per,)), hop, dma((n_fs,)), every, every, every, every, dma, dma((n_y,)),
             dma((n_y,)), dma((n_y,)), dma((n_y,))]
    hops = dma((2 * (n_fs - 1) * CUTS,))
    spread = dma((2 * (n_fs // 2) * 2,))
    served = [jax.ShapeDtypeStruct((2, hidden, model), kept), jax.ShapeDtypeStruct((hidden, model), kept)]
    vmem = pltpu.VMEM
    folded, down = vmem((2, wide, rows), kept), vmem(first[2].shape, kept)
    bounce = vmem((n_y - 1, 2, per, hidden // n_y, rows), kept)
    return pl.pallas_call(
        functools.partial(kernel, n_fs, n_tp),
        out_shape=served + served + [jax.ShapeDtypeStruct((share, model), kept)],
        in_specs=[pl.BlockSpec(memory_space=vmem)] * 3 + [pl.BlockSpec(memory_space=pltpu.HBM)] * 6,
        out_specs=[pl.BlockSpec(memory_space=vmem)] * 5,
        scratch_shapes=[
            vmem((2, rows, wide), first[0].dtype), vmem(first[2].shape, first[2].dtype),
            folded, folded, down, down, bounce, bounce,
            vmem((count, model), kept), vmem((count, model), kept), vmem((count, hidden), kept),
            vmem((share, model), kept), vmem((2, n_fs - 1, share, model // 2), kept), dma((6,)),
        ] + trade + trade + [hops] * 4 + [spread] * 2,
        compiler_params=pltpu.CompilerParams(
            collective_id=0, has_side_effects=True, vmem_limit_bytes=VMEM_LIMIT
        ),
        cost_estimate=pl.CostEstimate(
            flops=12 * count * model * hidden, bytes_accessed=48 * count * model, transcendentals=0
        ),
    )(tokens, *gains, *map(stay, first + second))


def place_kernel(gu_a, dn_a, gu_b, dn_b, done, *refs):
    outs, sems = refs[:-1], refs[-1]
    sources = (gu_a.at[0], gu_a.at[1], dn_a, gu_b.at[0], gu_b.at[1], dn_b, done)
    copies = [pltpu.make_async_copy(src, dst, sems.at[i]) for i, (src, dst) in enumerate(zip(sources, outs))]
    for copy in copies:
        copy.start()
    for copy in copies:
        copy.wait()


def place_results(gu_a, dn_a, gu_b, dn_b, done):
    block = jax.ShapeDtypeStruct(dn_a.shape, dn_a.dtype)
    outs = [block] * 6 + [jax.ShapeDtypeStruct(done.shape, done.dtype)]
    return pl.pallas_call(
        place_kernel,
        out_shape=outs,
        in_specs=[pl.BlockSpec(memory_space=pltpu.VMEM)] * 5,
        out_specs=[pl.BlockSpec(memory_space=pltpu.HBM)] * 7,
        scratch_shapes=[pltpu.SemaphoreType.DMA((7,))],
        compiler_params=pltpu.CompilerParams(vmem_limit_bytes=2**20),
    )(gu_a, dn_a, gu_b, dn_b, done)


def per_device(
    prompts,
    gain_first,
    gate_first,
    up_first,
    down_first,
    gain_second,
    gate_second,
    up_second,
    down_second,
):
    tokens = prompts.reshape(-1, prompts.shape[-1])
    gate_a, up_a, down_a, gate_b, up_b, down_b, finished = place_results(*both_half_steps(
        tokens, (gain_first[None], gain_second[None]),
        (gate_first, up_first, down_first), (gate_second, up_second, down_second),
    ))
    return (
        gate_a.T,
        up_a.T,
        down_a,
        gate_b.T,
        up_b.T,
        down_b,
        finished.reshape(prompts.shape[0], -1, prompts.shape[-1]),
    )


def solution(mesh):
    in_specs = (
        P("tp", None, None),
        P("fs"),
        P("fs", "tp"),
        P("fs", "tp"),
        P("fs", "tp"),
        P("fs"),
        P("fs", "tp"),
        P("fs", "tp"),
        P("fs", "tp"),
    )
    out_specs = (
        P(None, "fs"),
        P(None, "fs"),
        P("fs", None),
        P(None, "fs"),
        P(None, "fs"),
        P("fs", None),
        P("tp", "fs", None),
    )
    return jax.shard_map(
        per_device, mesh=mesh, in_specs=in_specs, out_specs=out_specs, check_vma=False
    )
```

```python
import functools

import jax
import jax.numpy as jnp
from jax import lax
from jax.experimental import pallas as pl
from jax.experimental.pallas import tpu as pltpu
from jax.sharding import PartitionSpec as P

CORES = 2
CUTS = 2
TILE = 256


def partner(index, step, count):
    if count & (count - 1):
        return (index + step) % count
    result, bit = 0, 1
    while bit < count:
        result = result + ((index // bit + step // bit) % 2) * bit
        bit *= 2
    return result


def tiles(total, size):
    return [(start, min(size, total - start)) for start in range(0, total, size)]


class Ring:
    def __init__(self, n_z, n_x):
        self.n_z, self.n_x, self.n = n_z, n_x, n_z * n_x

    def position(self, z, x):
        if self.n_x == 1:
            return z
        row, wide = self.n_z - 1 - z, self.n_x - 1
        back = self.n_z + row * wide + jnp.where(row % 2 == 0, x - 1, self.n_x - 1 - x)
        return jnp.where(x == 0, z, back)

    def at(self, place):
        place = (place + self.n) % self.n
        if self.n_x == 1:
            return place
        wide = self.n_x - 1
        rest = place + self.n - self.n_z
        row = (rest - self.n) // wide
        col = (rest - self.n) % wide
        back = (self.n_z - 1 - row) * self.n_x + jnp.where(row % 2 == 0, 1 + col, self.n_x - 1 - col)
        return jnp.where(place < self.n_z, place * self.n_x, back)

    def slot(self, offset):
        offset = offset % self.n
        if offset == 0:
            return 0
        if 2 * offset == self.n:
            return 1
        return 2 * offset + 1 if 2 * offset < self.n else 2 * (self.n - offset)


def remote(src, dst, send, recv, f, t):
    return pltpu.make_async_remote_copy(
        src_ref=src, dst_ref=dst, send_sem=send, recv_sem=recv,
        device_id={"fs": f, "tp": t}, device_id_type=pl.DeviceIdType.MESH,
    )


class Exchange:
    def __init__(self, n_fs, n_tp, gu, dn, gu_out, dn_out, bounce, sems):
        (self.send_c, self.recv_c, self.send_n, self.send_f, self.recv_a, self.send_y, self.recv_y,
         self.send_m, self.recv_m, self.dn_local, self.dn_send_y, self.dn_recv_y, self.dn_send_m,
         self.dn_recv_m) = sems
        self.n_fs, self.n_tp, self.n_y = n_fs, n_tp, n_tp // CORES
        self.per = n_fs // n_tp
        self.gu, self.dn, self.gu_out, self.dn_out, self.bounce = gu, dn, gu_out, dn_out, bounce
        self.hidden, self.rows = gu.shape[1] // self.per, gu.shape[2]
        self.part = self.hidden // self.n_y
        self.me_f, self.me_t = lax.axis_index("fs"), lax.axis_index("tp")
        self.my_y, self.my_c = self.me_t // CORES, self.me_t % CORES
        self.mate = self.my_y * CORES + (1 - self.my_c)
        self.at_home = self.me_f // self.per // CORES == self.my_y

    def peer(self, step):
        return (self.my_y + step) % self.n_y

    def beside(self, step):
        return self.peer(step) * CORES + self.my_c

    def window(self, f, y, c):
        return self.gu_out.at[c, pl.ds(pl.multiple_of(y * self.part, 8), self.part),
                              pl.ds(pl.multiple_of(f * self.rows, 128), self.rows)]

    def own(self, kind, i, y):
        return self.gu.at[kind, pl.ds(pl.multiple_of(i * self.hidden + y * self.part, 8), self.part), :]

    def cross(self, hop, kind, i):
        sem = ((hop - 1) * 2 + kind) * self.per + i
        return remote(self.own(kind, i, self.peer(hop)), self.bounce.at[hop - 1, kind, i],
                      self.send_c.at[sem], self.recv_c.at[sem], self.me_f, self.beside(hop))

    def start_cross(self, kind):
        for hop in range(1, self.n_y):
            for i in range(self.per):
                self.cross(hop, kind, i).start()

    def deliver(self, src, send, t, kind, i, act):
        f = t * self.per + i
        dst = self.window(self.me_f, self.my_y, kind)
        recv = self.recv_a.at[self.me_f]
        here = jnp.logical_and(f == self.me_f, kind == self.my_c)

        @pl.when(jnp.logical_not(here))
        def _():
            copy = remote(src, dst, send, recv, f, self.my_y * CORES + kind)
            copy.start() if act else copy.wait_send()

        if act:
            @pl.when(here)
            def _():
                pltpu.make_async_copy(src, dst, recv).start()

    def near(self, kind, act=True):
        for i in range(self.per):
            self.deliver(self.own(kind, i, self.my_y), self.send_n.at[kind * self.per + i], self.me_t,
                         kind, i, act)

    def pass_cross(self, act=True):
        for kind in range(2):
            for hop in range(1, self.n_y):
                for i in range(self.per):
                    sem = ((hop - 1) * 2 + kind) * self.per + i
                    held = self.bounce.at[self.n_y - hop - 1, kind, i]
                    came = ((self.n_y - hop - 1) * 2 + kind) * self.per + i
                    if act:
                        remote(held, held, self.send_c.at[came], self.recv_c.at[came], self.me_f,
                               self.mate).wait_recv()
                    self.deliver(held, self.send_f.at[sem], self.beside(hop), kind, i, act)

    def columns(self, t):
        width = self.dn.shape[1]
        return self.dn_out.at[:, pl.ds(pl.multiple_of(t * width, 128), width)]

    def dn_first(self):
        mine = self.columns(self.me_t)
        copies = [remote(self.dn, mine, self.dn_send_y.at[step], self.dn_recv_y.at[self.my_y],
                         self.me_f, self.beside(step)) for step in range(1, self.n_y)]
        copies.append(remote(self.dn, mine, self.dn_send_m.at[0], self.dn_recv_m.at[self.my_y],
                             self.me_f, self.mate))
        return copies

    def start_dn(self):
        self.keep = pltpu.make_async_copy(self.dn, self.columns(self.me_t), self.dn_local)
        self.keep.start()
        for copy in self.dn_first():
            copy.start()

    def on_first(self, step):
        f = partner(self.me_f, step, self.n_fs)
        piece = self.window(f, self.my_y, self.my_c)
        slot = self.my_y * self.n_fs + f
        copies = [remote(piece, piece, self.send_y.at[(hop - 1) * self.n_fs + step], self.recv_y.at[slot],
                         self.me_f, self.beside(hop)) for hop in range(1, self.n_y)]
        copies.append(remote(piece, piece, self.send_m.at[step], self.recv_m.at[slot], self.me_f, self.mate))
        return f, piece, copies

    def pass_first(self, steps):
        for step in steps:
            f, piece, copies = self.on_first(step)
            remote(piece, piece, self.send_m.at[0], self.recv_a.at[f], self.me_f, self.mate).wait_recv()
            for copy in copies:
                copy.start()

    def on_dn(self, hop):
        y = self.peer(hop)
        block = self.columns(y * CORES + self.my_c)
        return y, block, remote(block, block, self.dn_send_m.at[hop], self.dn_recv_m.at[y], self.me_f, self.mate)

    def pass_dn(self):
        for hop in range(1, self.n_y):
            y, block, copy = self.on_dn(hop)
            remote(block, block, self.dn_send_m.at[hop], self.dn_recv_y.at[y], self.me_f, self.mate).wait_recv()
            copy.start()

    def on_second(self, step, hop):
        f, y = partner(self.me_f, step, self.n_fs), self.peer(hop)
        piece = self.window(f, y, self.my_c)
        slot = y * self.n_fs + f
        send = self.send_m.at[hop * self.n_fs + step]
        return slot, piece, send, remote(piece, piece, send, self.recv_m.at[slot], self.me_f, self.mate)

    def pass_second(self):
        for step in range(self.n_fs):
            for hop in range(1, self.n_y):
                slot, piece, send, copy = self.on_second(step, hop)
                remote(piece, piece, send, self.recv_y.at[slot], self.me_f, self.mate).wait_recv()
                copy.start()

    def arrive_gu(self):
        for hop in range(self.n_y):
            y = self.peer(hop)
            for step in range(self.n_fs):
                f = partner(self.me_f, step, self.n_fs)
                piece = self.window(f, y, 1 - self.my_c)
                remote(piece, piece, self.send_m.at[0], self.recv_m.at[y * self.n_fs + f],
                       self.me_f, self.mate).wait_recv()

    def arrive_dn(self):
        for hop in range(self.n_y):
            y = self.peer(hop)
            block = self.columns(y * CORES + (1 - self.my_c))
            remote(block, block, self.dn_send_m.at[0], self.dn_recv_m.at[y], self.me_f, self.mate).wait_recv()
        self.keep.wait()

    def drain(self):
        for kind in range(2):
            for hop in range(1, self.n_y):
                for i in range(self.per):
                    self.cross(hop, kind, i).wait_send()
            self.near(kind, False)
        self.pass_cross(False)
        copies = self.dn_first() + [self.on_dn(hop)[2] for hop in range(1, self.n_y)]
        for step in range(self.n_fs):
            copies += self.on_first(step)[2] + [self.on_second(step, hop)[3] for hop in range(1, self.n_y)]
        for copy in copies:
            copy.wait_send()


class Reduce:
    def __init__(self, ring, place, part, landing, send, recv):
        self.ring, self.part, self.landing = ring, part, landing
        self.send, self.recv = send, recv
        self.me_t = lax.axis_index("tp")
        self.goes = (ring.at(place + 1), ring.at(place - 1))
        self.share = part.shape[0] // ring.n
        self.half = part.shape[1] // 2
        self.width = self.half // CUTS
        self.sends = []

    def mine(self, way, offset, k):
        slot = self.ring.slot(offset)
        return (pl.ds(slot * self.share, self.share), pl.ds(way * self.half + k * self.width, self.width))

    def land(self, way, s, k):
        return self.landing.at[way, s, :, pl.ds(k * self.width, self.width)]

    def sem(self, way, s, k):
        return (way * (self.ring.n - 1) + s) * CUTS + k

    def arrived(self, way, s, k):
        spot, sem = self.land(way, s, k), self.sem(way, s, k)
        remote(spot, spot, self.send.at[sem], self.recv.at[sem], self.goes[way], self.me_t).wait_recv()
        return spot[...].astype(jnp.float32)

    def step(self, s):
        for k in range(CUTS):
            for way in range(2):
                rows, cols = self.mine(way, -(1 + s) if way == 0 else 1 + s, k)
                if s > 0:
                    total = self.arrived(way, s - 1, k) + self.part[rows, cols].astype(jnp.float32)
                    self.part[rows, cols] = total.astype(self.part.dtype)
                sem = self.sem(way, s, k)
                self.sends.append(remote(self.part.at[rows, cols], self.land(way, s, k), self.send.at[sem],
                                         self.recv.at[sem], self.goes[way], self.me_t))
                self.sends[-1].start()

    def last(self, store):
        for k in range(CUTS):
            for way in range(2):
                rows, cols = self.mine(way, 0, k)
                total = self.arrived(way, self.ring.n - 2, k) + self.part[rows, cols].astype(jnp.float32)
                store(cols, total)


class Gather:
    def __init__(self, ring, place, blocks, send, recv):
        self.ring, self.blocks, self.send, self.recv = ring, blocks, send, recv
        self.me_t = lax.axis_index("tp")
        self.goes = (ring.at(place + 1), ring.at(place - 1))
        self.share = blocks.shape[0] // ring.n
        self.half = blocks.shape[1] // 2
        self.far = ring.n // 2
        self.sends = []

    def spot(self, offset, k):
        slot = self.ring.slot(offset)
        return self.blocks.at[pl.ds(slot * self.share, self.share), pl.ds(k * self.half, self.half)]

    def copy(self, way, s, k):
        sign = -1 if way == 0 else 1
        sem = (way * self.far + s) * 2 + k
        return remote(self.spot(sign * s, k), self.spot(sign * (s + 1), k), self.send.at[sem],
                      self.recv.at[sem], self.goes[way], self.me_t)

    def halves(self, way, s):
        return (0, 1) if s < self.far - 1 else (way,)

    def step(self, s):
        for k in range(2):
            for way in range(2):
                if s > 0:
                    self.copy(way, s - 1, k).wait_recv()
                if k in self.halves(way, s):
                    self.sends.append(self.copy(way, s, k))
                    self.sends[-1].start()

    def last(self):
        for way in range(2):
            self.copy(way, self.far - 1, way).wait_recv()


def normalize(rows):
    return (rows * lax.rsqrt(jnp.mean(rows * rows, axis=-1, keepdims=True) + 1e-06)).astype(jnp.bfloat16)


def active_rows(x, gu, act, start, count):
    rows = pl.ds(start, count)
    lanes = (((1,), (1,)), ((), ()))
    for at, size in tiles(gu.shape[1], TILE):
        gate = lax.dot_general(x[rows, :], gu[0, pl.ds(at, size), :], lanes, preferred_element_type=jnp.float32)
        up = lax.dot_general(x[rows, :], gu[1, pl.ds(at, size), :], lanes, preferred_element_type=jnp.float32)
        act[rows, pl.ds(at, size)] = (jax.nn.silu(gate) * up).astype(act.dtype)


def down_rows(act, dn, part, start, count):
    rows = pl.ds(start, count)
    for at, size in tiles(dn.shape[1], 2 * TILE):
        part[rows, pl.ds(at, size)] = jnp.dot(
            act[rows, :], dn[:, pl.ds(at, size)], preferred_element_type=jnp.float32
        ).astype(part.dtype)


def fold(staged, gain, kind, gu):
    count = staged.shape[2]

    def turn(cols, size):
        gu[kind, pl.ds(cols, size), :] = (staged[kind, :, pl.ds(cols, size)].T * gain[...]).astype(gu.dtype)

    @pl.loop(0, count // LANES)
    def _(j):
        turn(pl.multiple_of(j * LANES, LANES), LANES)

    if count % LANES:
        turn(count - count % LANES, count % LANES)


def kernel(n_fs, n_tp, tok, gain_a, gain_b, gate_a, up_a, down_a, gate_b, up_b, down_b,
           gu_out_a, dn_out_a, gu_out_b, dn_out_b, done,
           staged, staged_dn, scale_a, scale_b, gu_a, gu_b, dn_a, dn_b, bounce_a, bounce_b,
           x, part, act, mid, landing, load_sems, *sems):
    n_x = n_tp // CORES
    ring = Ring(n_fs // n_x, n_x)
    me_f, me_t = lax.axis_index("fs"), lax.axis_index("tp")
    place = ring.position(me_f // n_x, me_f % n_x)
    n, far = ring.n, ring.n // 2
    share = tok.shape[0] // n
    each = TRADE_SEMS
    one = Exchange(n_fs, n_tp, gu_a, dn_a, gu_out_a, dn_out_a, bounce_a, sems[:each])
    two = Exchange(n_fs, n_tp, gu_b, dn_b, gu_out_b, dn_out_b, bounce_b, sems[each:2 * each])
    rest = sems[2 * each:]
    sum_one = Reduce(ring, place, part, landing, rest[0], rest[1])
    sum_two = Reduce(ring, place, part, landing, rest[2], rest[3])
    spread = Gather(ring, place, x, rest[4], rest[5])

    def load(first, *pairs):
        copies = [pltpu.make_async_copy(src, dst, load_sems.at[first + i]) for i, (src, dst) in enumerate(pairs)]
        for copy in copies:
            copy.start()
        return copies

    own = pl.ds(pl.multiple_of(me_f * share, share), share)

    scales = load(0, (gain_a, scale_a), (gain_b, scale_b))
    loads = load(2, (gate_a, staged.at[0]), (up_a, staged.at[1]), (down_a, staged_dn))
    rows_in = load(5, (tok, part), (tok.at[own, :], mid))

    barrier = pltpu.get_barrier_semaphore()

    def greet(f, t):
        pl.semaphore_signal(
            barrier, inc=1, device_id={"fs": f, "tp": t}, device_id_type=pl.DeviceIdType.MESH
        )

    core = me_f // one.per % CORES
    is_self = core == one.my_c
    for step in range(n_fs):
        f = partner(me_f, step, n_fs)
        if step == 0:
            @pl.when(jnp.logical_not(is_self))
            def _():
                greet(f, one.my_y * CORES + core)
        else:
            greet(f, one.my_y * CORES + core)
    for step in range(1, one.n_y):
        greet(me_f, one.beside(step))
    greet(me_f, one.mate)
    greet(ring.at(place + 1), me_t)
    greet(ring.at(place - 1), me_t)
    pl.semaphore_wait(barrier, n_fs + one.n_y + 2 - jnp.where(is_self, 1, 0))

    for copy in scales:
        copy.wait()
    for kind in range(2):
        loads[kind].wait()
        fold(staged, scale_a, kind, gu_a)
        one.start_cross(kind)
        one.near(kind)
    loads[2].wait()
    dn_a[...] = staged_dn[...].astype(dn_a.dtype)
    loads = load(7, (gate_b, staged.at[0]), (up_b, staged.at[1]), (down_b, staged_dn))
    for copy in rows_in:
        copy.wait()

    @pl.loop(0, n)
    def _(j):
        sign = jnp.where(j % 2 == 0, -1, 1)
        offset = jnp.where(j < 2, j * far, sign * (j // 2))
        f = ring.at(place + offset)
        rows = part[pl.ds(pl.multiple_of(f * share, share), share), :].astype(jnp.float32)
        x[pl.ds(pl.multiple_of(j * share, share), share), :] = normalize(rows)

    for kind in range(2):
        loads[kind].wait()
        fold(staged, scale_b, kind, gu_b)
        two.start_cross(kind)
        two.near(kind)
    loads[2].wait()
    dn_b[...] = staged_dn[...].astype(dn_b.dtype)

    one.pass_cross()
    one.pass_first(range(n_fs // 2))
    two.pass_cross()
    one.pass_first(range(n_fs // 2, n_fs))
    one.start_dn()
    one.pass_second()
    one.arrive_gu()

    @pl.loop(0, far)
    def _(j):
        active_rows(x, gu_out_a, act, pl.multiple_of(j * 2 * share, 2 * share), 2 * share)

    two.start_dn()
    one.pass_dn()
    one.arrive_dn()
    for s in range(n - 1):
        if s < far:
            down_rows(act, dn_out_a, part, 2 * ((s + 1) % far) * share, 2 * share)
        sum_one.step(s)
        if s == far - 3:
            two.pass_first(range(n_fs // 2))
        if s == far - 1:
            two.pass_first(range(n_fs // 2, n_fs))

    def store_middle(cols, total):
        mid[:, cols] = (mid[:, cols].astype(jnp.float32) + 0.5 * total).astype(mid.dtype)

    sum_one.last(store_middle)
    x[pl.ds(0, share), :] = normalize(mid[...].astype(jnp.float32))

    spread.step(0)
    two.pass_dn()
    for copy in sum_one.sends:
        copy.wait_send()
    spread.step(1)
    two.pass_second()
    two.arrive_gu()
    two.arrive_dn()
    for s in range(1, far):
        if s > 1:
            spread.step(s)
        active_rows(x, gu_out_b, act, 2 * s * share, 2 * share)
        down_rows(act, dn_out_b, part, 2 * s * share, 2 * share)
        sum_two.step(s - 1)
    spread.last()
    active_rows(x, gu_out_b, act, 0, 2 * share)
    down_rows(act, dn_out_b, part, 0, 2 * share)
    for s in range(far - 1, n - 1):
        sum_two.step(s)

    def store_done(cols, total):
        done[:, cols] = (mid[:, cols].astype(jnp.float32) + 0.5 * total).astype(done.dtype)

    sum_two.last(store_done)

    one.drain()
    two.drain()
    for copy in spread.sends + sum_two.sends:
        copy.wait_send()


TRADE_SEMS = 14
LANES = 128
VMEM_LIMIT = 32 * 2**20


def stay(array):
    return pltpu.with_memory_space_constraint(array, pltpu.HBM)


def both_half_steps(tokens, gains, first, second):
    n_fs, n_tp = lax.axis_size("fs"), lax.axis_size("tp")
    n_y, per = n_tp // CORES, n_fs // n_tp
    count, model = tokens.shape
    rows, wide = first[0].shape
    share, hidden = count // n_fs, wide // per
    kept = tokens.dtype
    dma = pltpu.SemaphoreType.DMA
    hop, every = dma(((n_y - 1) * 2 * per,)), dma((n_y * n_fs,))
    trade = [hop, hop, dma((2 * per,)), hop, dma((n_fs,)), every, every, every, every, dma, dma((n_y,)),
             dma((n_y,)), dma((n_y,)), dma((n_y,))]
    hops = dma((2 * (n_fs - 1) * CUTS,))
    spread = dma((2 * (n_fs // 2) * 2,))
    served = [jax.ShapeDtypeStruct((2, hidden, model), kept), jax.ShapeDtypeStruct((hidden, model), kept)]
    vmem = pltpu.VMEM
    folded, down = vmem((2, wide, rows), kept), vmem(first[2].shape, kept)
    bounce = vmem((n_y - 1, 2, per, hidden // n_y, rows), kept)
    return pl.pallas_call(
        functools.partial(kernel, n_fs, n_tp),
        out_shape=served + served + [jax.ShapeDtypeStruct((share, model), kept)],
        in_specs=[pl.BlockSpec(memory_space=pltpu.HBM)] * 9,
        out_specs=[pl.BlockSpec(memory_space=vmem)] * 5,
        scratch_shapes=[
            vmem((2, rows, wide), first[0].dtype), vmem(first[2].shape, first[2].dtype),
            vmem(gains[0].shape, gains[0].dtype), vmem(gains[1].shape, gains[1].dtype), folded, folded, down, down, bounce, bounce,
            vmem((count, model), kept), vmem((count, model), kept), vmem((count, hidden), kept),
            vmem((share, model), kept), vmem((2, n_fs - 1, share, model // 2), kept), dma((10,)),
        ] + trade + trade + [hops] * 4 + [spread] * 2,
        compiler_params=pltpu.CompilerParams(
            collective_id=0, has_side_effects=True, vmem_limit_bytes=VMEM_LIMIT
        ),
        cost_estimate=pl.CostEstimate(
            flops=12 * count * model * hidden, bytes_accessed=48 * count * model, transcendentals=0
        ),
    )(*map(stay, (tokens,) + gains + first + second))


def place_kernel(gu_a, dn_a, gu_b, dn_b, done, *refs):
    outs, sems = refs[:-1], refs[-1]
    sources = (gu_a.at[0], gu_a.at[1], dn_a, gu_b.at[0], gu_b.at[1], dn_b, done)
    copies = [pltpu.make_async_copy(src, dst, sems.at[i]) for i, (src, dst) in enumerate(zip(sources, outs))]
    for copy in copies:
        copy.start()
    for copy in copies:
        copy.wait()


def place_results(gu_a, dn_a, gu_b, dn_b, done):
    block = jax.ShapeDtypeStruct(dn_a.shape, dn_a.dtype)
    outs = [block] * 6 + [jax.ShapeDtypeStruct(done.shape, done.dtype)]
    return pl.pallas_call(
        place_kernel,
        out_shape=outs,
        in_specs=[pl.BlockSpec(memory_space=pltpu.VMEM)] * 5,
        out_specs=[pl.BlockSpec(memory_space=pltpu.HBM)] * 7,
        scratch_shapes=[pltpu.SemaphoreType.DMA((7,))],
        compiler_params=pltpu.CompilerParams(vmem_limit_bytes=2**20),
    )(gu_a, dn_a, gu_b, dn_b, done)


def per_device(
    prompts,
    gain_first,
    gate_first,
    up_first,
    down_first,
    gain_second,
    gate_second,
    up_second,
    down_second,
):
    tokens = prompts.reshape(-1, prompts.shape[-1])
    gate_a, up_a, down_a, gate_b, up_b, down_b, finished = place_results(*both_half_steps(
        tokens, (gain_first[None], gain_second[None]),
        (gate_first, up_first, down_first), (gate_second, up_second, down_second),
    ))
    return (
        gate_a.T,
        up_a.T,
        down_a,
        gate_b.T,
        up_b.T,
        down_b,
        finished.reshape(prompts.shape[0], -1, prompts.shape[-1]),
    )


def solution(mesh):
    in_specs = (
        P("tp", None, None),
        P("fs"),
        P("fs", "tp"),
        P("fs", "tp"),
        P("fs", "tp"),
        P("fs"),
        P("fs", "tp"),
        P("fs", "tp"),
        P("fs", "tp"),
    )
    out_specs = (
        P(None, "fs"),
        P(None, "fs"),
        P("fs", None),
        P(None, "fs"),
        P(None, "fs"),
        P("fs", None),
        P("tp", "fs", None),
    )
    return jax.shard_map(
        per_device, mesh=mesh, in_specs=in_specs, out_specs=out_specs, check_vma=False
    )
```

```python
import functools

import jax
import jax.numpy as jnp
from jax import lax
from jax.experimental import pallas as pl
from jax.experimental.pallas import tpu as pltpu
from jax.sharding import PartitionSpec as P

CORES = 2
CUTS = 2
TILE = 256


def partner(index, step, count):
    if count & (count - 1):
        return (index + step) % count
    result, bit = 0, 1
    while bit < count:
        result = result + ((index // bit + step // bit) % 2) * bit
        bit *= 2
    return result


def tiles(total, size):
    return [(start, min(size, total - start)) for start in range(0, total, size)]


class Ring:
    def __init__(self, n_z, n_x):
        self.n_z, self.n_x, self.n = n_z, n_x, n_z * n_x

    def position(self, z, x):
        if self.n_x == 1:
            return z
        row, wide = self.n_z - 1 - z, self.n_x - 1
        back = self.n_z + row * wide + jnp.where(row % 2 == 0, x - 1, self.n_x - 1 - x)
        return jnp.where(x == 0, z, back)

    def at(self, place):
        place = (place + self.n) % self.n
        if self.n_x == 1:
            return place
        wide = self.n_x - 1
        rest = place + self.n - self.n_z
        row = (rest - self.n) // wide
        col = (rest - self.n) % wide
        back = (self.n_z - 1 - row) * self.n_x + jnp.where(row % 2 == 0, 1 + col, self.n_x - 1 - col)
        return jnp.where(place < self.n_z, place * self.n_x, back)

    def slot(self, offset):
        offset = offset % self.n
        if offset == 0:
            return 0
        if 2 * offset == self.n:
            return 1
        return 2 * offset + 1 if 2 * offset < self.n else 2 * (self.n - offset)


def remote(src, dst, send, recv, f, t):
    return pltpu.make_async_remote_copy(
        src_ref=src, dst_ref=dst, send_sem=send, recv_sem=recv,
        device_id={"fs": f, "tp": t}, device_id_type=pl.DeviceIdType.MESH,
    )


class Exchange:
    def __init__(self, n_fs, n_tp, gu, dn, gu_out, dn_out, bounce, sems):
        (self.send_c, self.recv_c, self.send_n, self.send_f, self.recv_a, self.send_y, self.recv_y,
         self.send_m, self.recv_m, self.dn_local, self.dn_send_y, self.dn_recv_y, self.dn_send_m,
         self.dn_recv_m) = sems
        self.n_fs, self.n_tp, self.n_y = n_fs, n_tp, n_tp // CORES
        self.per = n_fs // n_tp
        self.gu, self.dn, self.gu_out, self.dn_out, self.bounce = gu, dn, gu_out, dn_out, bounce
        self.hidden, self.rows = gu.shape[1] // self.per, gu.shape[2]
        self.part = self.hidden // self.n_y
        self.me_f, self.me_t = lax.axis_index("fs"), lax.axis_index("tp")
        self.my_y, self.my_c = self.me_t // CORES, self.me_t % CORES
        self.mate = self.my_y * CORES + (1 - self.my_c)
        self.at_home = self.me_f // self.per // CORES == self.my_y

    def peer(self, step):
        return (self.my_y + step) % self.n_y

    def beside(self, step):
        return self.peer(step) * CORES + self.my_c

    def window(self, f, y, c):
        return self.gu_out.at[c, pl.ds(pl.multiple_of(y * self.part, 8), self.part),
                              pl.ds(pl.multiple_of(f * self.rows, 128), self.rows)]

    def own(self, kind, i, y):
        return self.gu.at[kind, pl.ds(pl.multiple_of(i * self.hidden + y * self.part, 8), self.part), :]

    def cross(self, hop, kind, i):
        sem = ((hop - 1) * 2 + kind) * self.per + i
        return remote(self.own(kind, i, self.peer(hop)), self.bounce.at[hop - 1, kind, i],
                      self.send_c.at[sem], self.recv_c.at[sem], self.me_f, self.beside(hop))

    def start_cross(self, kind, i):
        for hop in range(1, self.n_y):
            self.cross(hop, kind, i).start()

    def deliver(self, src, send, t, kind, i, act):
        f = t * self.per + i
        dst = self.window(self.me_f, self.my_y, kind)
        recv = self.recv_a.at[self.me_f]
        here = jnp.logical_and(f == self.me_f, kind == self.my_c)

        @pl.when(jnp.logical_not(here))
        def _():
            copy = remote(src, dst, send, recv, f, self.my_y * CORES + kind)
            copy.start() if act else copy.wait_send()

        if act:
            @pl.when(here)
            def _():
                pltpu.make_async_copy(src, dst, recv).start()

    def near(self, kind, i, act=True):
        self.deliver(self.own(kind, i, self.my_y), self.send_n.at[kind * self.per + i], self.me_t,
                     kind, i, act)

    def fold_and_send(self, staged, gain, kind):
        done, wide = 0, self.gu.shape[1]
        for i in range(self.per):
            stop = min(wide, -(-(i + 1) * self.hidden // LANES) * LANES)
            fold(staged, gain, kind, self.gu, done, stop)
            done = stop
            self.start_cross(kind, i)
            self.near(kind, i)

    def pass_cross(self, act=True):
        for kind in range(2):
            for hop in range(1, self.n_y):
                for i in range(self.per):
                    sem = ((hop - 1) * 2 + kind) * self.per + i
                    held = self.bounce.at[self.n_y - hop - 1, kind, i]
                    came = ((self.n_y - hop - 1) * 2 + kind) * self.per + i
                    if act:
                        remote(held, held, self.send_c.at[came], self.recv_c.at[came], self.me_f,
                               self.mate).wait_recv()
                    self.deliver(held, self.send_f.at[sem], self.beside(hop), kind, i, act)

    def columns(self, t):
        width = self.dn.shape[1]
        return self.dn_out.at[:, pl.ds(pl.multiple_of(t * width, 128), width)]

    def dn_first(self):
        mine = self.columns(self.me_t)
        copies = [remote(self.dn, mine, self.dn_send_y.at[step], self.dn_recv_y.at[self.my_y],
                         self.me_f, self.beside(step)) for step in range(1, self.n_y)]
        copies.append(remote(self.dn, mine, self.dn_send_m.at[0], self.dn_recv_m.at[self.my_y],
                             self.me_f, self.mate))
        return copies

    def start_dn(self):
        self.keep = pltpu.make_async_copy(self.dn, self.columns(self.me_t), self.dn_local)
        self.keep.start()
        for copy in self.dn_first():
            copy.start()

    def on_first(self, step):
        f = partner(self.me_f, step, self.n_fs)
        piece = self.window(f, self.my_y, self.my_c)
        slot = self.my_y * self.n_fs + f
        copies = [remote(piece, piece, self.send_y.at[(hop - 1) * self.n_fs + step], self.recv_y.at[slot],
                         self.me_f, self.beside(hop)) for hop in range(1, self.n_y)]
        copies.append(remote(piece, piece, self.send_m.at[step], self.recv_m.at[slot], self.me_f, self.mate))
        return f, piece, copies

    def pass_first(self, steps):
        for step in steps:
            f, piece, copies = self.on_first(step)
            remote(piece, piece, self.send_m.at[0], self.recv_a.at[f], self.me_f, self.mate).wait_recv()
            for copy in copies:
                copy.start()

    def on_dn(self, hop):
        y = self.peer(hop)
        block = self.columns(y * CORES + self.my_c)
        return y, block, remote(block, block, self.dn_send_m.at[hop], self.dn_recv_m.at[y], self.me_f, self.mate)

    def pass_dn(self):
        for hop in range(1, self.n_y):
            y, block, copy = self.on_dn(hop)
            remote(block, block, self.dn_send_m.at[hop], self.dn_recv_y.at[y], self.me_f, self.mate).wait_recv()
            copy.start()

    def on_second(self, step, hop):
        f, y = partner(self.me_f, step, self.n_fs), self.peer(hop)
        piece = self.window(f, y, self.my_c)
        slot = y * self.n_fs + f
        send = self.send_m.at[hop * self.n_fs + step]
        return slot, piece, send, remote(piece, piece, send, self.recv_m.at[slot], self.me_f, self.mate)

    def pass_second(self):
        for step in range(self.n_fs):
            for hop in range(1, self.n_y):
                slot, piece, send, copy = self.on_second(step, hop)
                remote(piece, piece, send, self.recv_y.at[slot], self.me_f, self.mate).wait_recv()
                copy.start()

    def arrive_gu(self):
        for hop in range(self.n_y):
            y = self.peer(hop)
            for step in range(self.n_fs):
                f = partner(self.me_f, step, self.n_fs)
                piece = self.window(f, y, 1 - self.my_c)
                remote(piece, piece, self.send_m.at[0], self.recv_m.at[y * self.n_fs + f],
                       self.me_f, self.mate).wait_recv()

    def arrive_dn(self):
        for hop in range(self.n_y):
            y = self.peer(hop)
            block = self.columns(y * CORES + (1 - self.my_c))
            remote(block, block, self.dn_send_m.at[0], self.dn_recv_m.at[y], self.me_f, self.mate).wait_recv()
        self.keep.wait()

    def drain(self):
        for kind in range(2):
            for hop in range(1, self.n_y):
                for i in range(self.per):
                    self.cross(hop, kind, i).wait_send()
            for i in range(self.per):
                self.near(kind, i, False)
        self.pass_cross(False)
        copies = self.dn_first() + [self.on_dn(hop)[2] for hop in range(1, self.n_y)]
        for step in range(self.n_fs):
            copies += self.on_first(step)[2] + [self.on_second(step, hop)[3] for hop in range(1, self.n_y)]
        for copy in copies:
            copy.wait_send()


class Reduce:
    def __init__(self, ring, place, part, landing, send, recv):
        self.ring, self.part, self.landing = ring, part, landing
        self.send, self.recv = send, recv
        self.me_t = lax.axis_index("tp")
        self.goes = (ring.at(place + 1), ring.at(place - 1))
        self.share = part.shape[0] // ring.n
        self.half = part.shape[1] // 2
        self.width = self.half // CUTS
        self.sends = []

    def mine(self, way, offset, k):
        slot = self.ring.slot(offset)
        return (pl.ds(slot * self.share, self.share), pl.ds(way * self.half + k * self.width, self.width))

    def land(self, way, s, k):
        return self.landing.at[way, s, :, pl.ds(k * self.width, self.width)]

    def sem(self, way, s, k):
        return (way * (self.ring.n - 1) + s) * CUTS + k

    def arrived(self, way, s, k):
        spot, sem = self.land(way, s, k), self.sem(way, s, k)
        remote(spot, spot, self.send.at[sem], self.recv.at[sem], self.goes[way], self.me_t).wait_recv()
        return spot[...].astype(jnp.float32)

    def step(self, s):
        for k in range(CUTS):
            for way in range(2):
                rows, cols = self.mine(way, -(1 + s) if way == 0 else 1 + s, k)
                if s > 0:
                    total = self.arrived(way, s - 1, k) + self.part[rows, cols].astype(jnp.float32)
                    self.part[rows, cols] = total.astype(self.part.dtype)
                sem = self.sem(way, s, k)
                self.sends.append(remote(self.part.at[rows, cols], self.land(way, s, k), self.send.at[sem],
                                         self.recv.at[sem], self.goes[way], self.me_t))
                self.sends[-1].start()

    def last(self, store):
        for k in range(CUTS):
            for way in range(2):
                rows, cols = self.mine(way, 0, k)
                total = self.arrived(way, self.ring.n - 2, k) + self.part[rows, cols].astype(jnp.float32)
                store(cols, total)


class Gather:
    def __init__(self, ring, place, blocks, send, recv):
        self.ring, self.blocks, self.send, self.recv = ring, blocks, send, recv
        self.me_t = lax.axis_index("tp")
        self.goes = (ring.at(place + 1), ring.at(place - 1))
        self.share = blocks.shape[0] // ring.n
        self.half = blocks.shape[1] // 2
        self.far = ring.n // 2
        self.sends = []

    def spot(self, offset, k):
        slot = self.ring.slot(offset)
        return self.blocks.at[pl.ds(slot * self.share, self.share), pl.ds(k * self.half, self.half)]

    def copy(self, way, s, k):
        sign = -1 if way == 0 else 1
        sem = (way * self.far + s) * 2 + k
        return remote(self.spot(sign * s, k), self.spot(sign * (s + 1), k), self.send.at[sem],
                      self.recv.at[sem], self.goes[way], self.me_t)

    def halves(self, way, s):
        return (0, 1) if s < self.far - 1 else (way,)

    def step(self, s):
        for k in range(2):
            for way in range(2):
                if s > 0:
                    self.copy(way, s - 1, k).wait_recv()
                if k in self.halves(way, s):
                    self.sends.append(self.copy(way, s, k))
                    self.sends[-1].start()

    def last(self):
        for way in range(2):
            self.copy(way, self.far - 1, way).wait_recv()


def normalize(rows):
    return (rows * lax.rsqrt(jnp.mean(rows * rows, axis=-1, keepdims=True) + 1e-06)).astype(jnp.bfloat16)


def active_rows(x, gu, act, start, count):
    rows = pl.ds(start, count)
    lanes = (((1,), (1,)), ((), ()))
    for at, size in tiles(gu.shape[1], TILE):
        gate = lax.dot_general(x[rows, :], gu[0, pl.ds(at, size), :], lanes, preferred_element_type=jnp.float32)
        up = lax.dot_general(x[rows, :], gu[1, pl.ds(at, size), :], lanes, preferred_element_type=jnp.float32)
        act[rows, pl.ds(at, size)] = (jax.nn.silu(gate) * up).astype(act.dtype)


def down_rows(act, dn, part, start, count):
    rows = pl.ds(start, count)
    for at, size in tiles(dn.shape[1], 2 * TILE):
        part[rows, pl.ds(at, size)] = jnp.dot(
            act[rows, :], dn[:, pl.ds(at, size)], preferred_element_type=jnp.float32
        ).astype(part.dtype)


def fold(staged, gain, kind, gu, start, stop):
    count = stop - start

    def turn(cols, size):
        gu[kind, pl.ds(cols, size), :] = (staged[kind, :, pl.ds(cols, size)].T * gain[...]).astype(gu.dtype)

    @pl.loop(0, count // LANES)
    def _(j):
        turn(pl.multiple_of(start + j * LANES, LANES), LANES)

    if count % LANES:
        turn(stop - count % LANES, count % LANES)


def kernel(n_fs, n_tp, tok, gain_a, gain_b, gate_a, up_a, down_a, gate_b, up_b, down_b,
           gu_out_a, dn_out_a, gu_out_b, dn_out_b, done,
           staged, staged_dn, scale_a, scale_b, gu_a, gu_b, dn_a, dn_b, bounce_a, bounce_b,
           x, part, act, mid, landing, load_sems, *sems):
    n_x = n_tp // CORES
    ring = Ring(n_fs // n_x, n_x)
    me_f, me_t = lax.axis_index("fs"), lax.axis_index("tp")
    place = ring.position(me_f // n_x, me_f % n_x)
    n, far = ring.n, ring.n // 2
    share = tok.shape[0] // n
    each = TRADE_SEMS
    one = Exchange(n_fs, n_tp, gu_a, dn_a, gu_out_a, dn_out_a, bounce_a, sems[:each])
    two = Exchange(n_fs, n_tp, gu_b, dn_b, gu_out_b, dn_out_b, bounce_b, sems[each:2 * each])
    rest = sems[2 * each:]
    sum_one = Reduce(ring, place, part, landing, rest[0], rest[1])
    sum_two = Reduce(ring, place, part, landing, rest[2], rest[3])
    spread = Gather(ring, place, x, rest[4], rest[5])

    def load(first, *pairs):
        copies = [pltpu.make_async_copy(src, dst, load_sems.at[first + i]) for i, (src, dst) in enumerate(pairs)]
        for copy in copies:
            copy.start()
        return copies

    own = pl.ds(pl.multiple_of(me_f * share, share), share)

    scales = load(0, (gain_a, scale_a), (gain_b, scale_b))
    loads = load(2, (gate_a, staged.at[0]), (up_a, staged.at[1]), (down_a, staged_dn))

    barrier = pltpu.get_barrier_semaphore()

    def greet(f, t):
        pl.semaphore_signal(
            barrier, inc=1, device_id={"fs": f, "tp": t}, device_id_type=pl.DeviceIdType.MESH
        )

    core = me_f // one.per % CORES
    is_self = core == one.my_c
    for step in range(n_fs):
        f = partner(me_f, step, n_fs)
        if step == 0:
            @pl.when(jnp.logical_not(is_self))
            def _():
                greet(f, one.my_y * CORES + core)
        else:
            greet(f, one.my_y * CORES + core)
    for step in range(1, one.n_y):
        greet(me_f, one.beside(step))
    greet(me_f, one.mate)
    greet(ring.at(place + 1), me_t)
    greet(ring.at(place - 1), me_t)
    pl.semaphore_wait(barrier, n_fs + one.n_y + 2 - jnp.where(is_self, 1, 0))

    for copy in scales:
        copy.wait()
    for kind in range(2):
        loads[kind].wait()
        one.fold_and_send(staged, scale_a, kind)
    rows_in = load(5, (tok, part), (tok.at[own, :], mid))
    loads[2].wait()
    dn_a[...] = staged_dn[...].astype(dn_a.dtype)
    loads = load(7, (gate_b, staged.at[0]), (up_b, staged.at[1]), (down_b, staged_dn))
    for copy in rows_in:
        copy.wait()

    @pl.loop(0, n)
    def _(j):
        sign = jnp.where(j % 2 == 0, -1, 1)
        offset = jnp.where(j < 2, j * far, sign * (j // 2))
        f = ring.at(place + offset)
        rows = part[pl.ds(pl.multiple_of(f * share, share), share), :].astype(jnp.float32)
        x[pl.ds(pl.multiple_of(j * share, share), share), :] = normalize(rows)

    for kind in range(2):
        loads[kind].wait()
        two.fold_and_send(staged, scale_b, kind)
    loads[2].wait()
    dn_b[...] = staged_dn[...].astype(dn_b.dtype)

    one.pass_cross()
    one.pass_first(range(n_fs // 2))
    two.pass_cross()
    one.pass_first(range(n_fs // 2, n_fs))
    one.start_dn()
    one.pass_second()
    one.arrive_gu()

    @pl.loop(0, far)
    def _(j):
        active_rows(x, gu_out_a, act, pl.multiple_of(j * 2 * share, 2 * share), 2 * share)

    two.start_dn()
    one.pass_dn()
    one.arrive_dn()
    for s in range(n - 1):
        if s < far:
            down_rows(act, dn_out_a, part, 2 * ((s + 1) % far) * share, 2 * share)
        sum_one.step(s)
        if s == far - 3:
            two.pass_first(range(n_fs // 2))
        if s == far - 1:
            two.pass_first(range(n_fs // 2, n_fs))

    def store_middle(cols, total):
        mid[:, cols] = (mid[:, cols].astype(jnp.float32) + 0.5 * total).astype(mid.dtype)

    sum_one.last(store_middle)
    x[pl.ds(0, share), :] = normalize(mid[...].astype(jnp.float32))

    spread.step(0)
    two.pass_dn()
    for copy in sum_one.sends:
        copy.wait_send()
    spread.step(1)
    two.pass_second()
    two.arrive_gu()
    two.arrive_dn()
    for s in range(1, far):
        if s > 1:
            spread.step(s)
        active_rows(x, gu_out_b, act, 2 * s * share, 2 * share)
        down_rows(act, dn_out_b, part, 2 * s * share, 2 * share)
        sum_two.step(s - 1)
    spread.last()
    active_rows(x, gu_out_b, act, 0, 2 * share)
    down_rows(act, dn_out_b, part, 0, 2 * share)
    for s in range(far - 1, n - 1):
        sum_two.step(s)

    def store_done(cols, total):
        done[:, cols] = (mid[:, cols].astype(jnp.float32) + 0.5 * total).astype(done.dtype)

    sum_two.last(store_done)

    one.drain()
    two.drain()
    for copy in spread.sends + sum_two.sends:
        copy.wait_send()


TRADE_SEMS = 14
LANES = 128
PIECES = 2
VMEM_LIMIT = 32 * 2**20


def stay(array):
    return pltpu.with_memory_space_constraint(array, pltpu.HBM)


def both_half_steps(tokens, gains, first, second):
    n_fs, n_tp = lax.axis_size("fs"), lax.axis_size("tp")
    n_y, per = n_tp // CORES, n_fs // n_tp
    count, model = tokens.shape
    rows, wide = first[0].shape
    share, hidden = count // n_fs, wide // per
    kept = tokens.dtype
    dma = pltpu.SemaphoreType.DMA
    hop, every = dma(((n_y - 1) * 2 * per,)), dma((n_y * n_fs,))
    trade = [hop, hop, dma((2 * per,)), hop, dma((n_fs,)), every, every, every, every, dma, dma((n_y,)),
             dma((n_y,)), dma((n_y,)), dma((n_y,))]
    hops = dma((2 * (n_fs - 1) * CUTS,))
    spread = dma((2 * (n_fs // 2) * 2,))
    served = [jax.ShapeDtypeStruct((2, hidden, model), kept), jax.ShapeDtypeStruct((hidden, model), kept)]
    vmem = pltpu.VMEM
    folded, down = vmem((2, wide, rows), kept), vmem(first[2].shape, kept)
    bounce = vmem((n_y - 1, 2, per, hidden // n_y, rows), kept)
    return pl.pallas_call(
        functools.partial(kernel, n_fs, n_tp),
        out_shape=served + served + [jax.ShapeDtypeStruct((share, model), kept)],
        in_specs=[pl.BlockSpec(memory_space=pltpu.HBM)] * 9,
        out_specs=[pl.BlockSpec(memory_space=vmem)] * 5,
        scratch_shapes=[
            vmem((2, rows, wide), first[0].dtype), vmem(first[2].shape, first[2].dtype),
            vmem(gains[0].shape, gains[0].dtype), vmem(gains[1].shape, gains[1].dtype), folded, folded, down, down, bounce, bounce,
            vmem((count, model), kept), vmem((count, model), kept), vmem((count, hidden), kept),
            vmem((share, model), kept), vmem((2, n_fs - 1, share, model // 2), kept), dma((10,)),
        ] + trade + trade + [hops] * 4 + [spread] * 2,
        compiler_params=pltpu.CompilerParams(
            collective_id=0, has_side_effects=True, vmem_limit_bytes=VMEM_LIMIT
        ),
        cost_estimate=pl.CostEstimate(
            flops=12 * count * model * hidden, bytes_accessed=48 * count * model, transcendentals=0
        ),
    )(*map(stay, (tokens,) + gains + first + second))


def place_kernel(gu_a, dn_a, gu_b, dn_b, done, *refs):
    outs, sems = refs[:-1], refs[-1]
    sources = (gu_a.at[0], gu_a.at[1], dn_a, gu_b.at[0], gu_b.at[1], dn_b, done)
    copies = []
    for src, dst in zip(sources, outs):
        rows = src.shape[0] // PIECES
        for j in range(PIECES):
            cut = pl.ds(j * rows, rows)
            copies.append(pltpu.make_async_copy(src.at[cut, :], dst.at[cut, :], sems.at[len(copies)]))
    for copy in copies:
        copy.start()
    for copy in copies:
        copy.wait()


def place_results(gu_a, dn_a, gu_b, dn_b, done):
    block = jax.ShapeDtypeStruct(dn_a.shape, dn_a.dtype)
    outs = [block] * 6 + [jax.ShapeDtypeStruct(done.shape, done.dtype)]
    return pl.pallas_call(
        place_kernel,
        out_shape=outs,
        in_specs=[pl.BlockSpec(memory_space=pltpu.VMEM)] * 5,
        out_specs=[pl.BlockSpec(memory_space=pltpu.HBM)] * 7,
        scratch_shapes=[pltpu.SemaphoreType.DMA((7 * PIECES,))],
        compiler_params=pltpu.CompilerParams(vmem_limit_bytes=2**20),
    )(gu_a, dn_a, gu_b, dn_b, done)


def per_device(
    prompts,
    gain_first,
    gate_first,
    up_first,
    down_first,
    gain_second,
    gate_second,
    up_second,
    down_second,
):
    tokens = prompts.reshape(-1, prompts.shape[-1])
    gate_a, up_a, down_a, gate_b, up_b, down_b, finished = place_results(*both_half_steps(
        tokens, (gain_first[None], gain_second[None]),
        (gate_first, up_first, down_first), (gate_second, up_second, down_second),
    ))
    return (
        gate_a.T,
        up_a.T,
        down_a,
        gate_b.T,
        up_b.T,
        down_b,
        finished.reshape(prompts.shape[0], -1, prompts.shape[-1]),
    )


def solution(mesh):
    in_specs = (
        P("tp", None, None),
        P("fs"),
        P("fs", "tp"),
        P("fs", "tp"),
        P("fs", "tp"),
        P("fs"),
        P("fs", "tp"),
        P("fs", "tp"),
        P("fs", "tp"),
    )
    out_specs = (
        P(None, "fs"),
        P(None, "fs"),
        P("fs", None),
        P(None, "fs"),
        P(None, "fs"),
        P("fs", None),
        P("tp", "fs", None),
    )
    return jax.shard_map(
        per_device, mesh=mesh, in_specs=in_specs, out_specs=out_specs, check_vma=False
    )
```
